256 devices in a mesh: kv: 32 (over z, y), tp: 8 (over x, core).
Axes of the slice: x: 4, y: 4, z: 8, core: 2. Of those that a mesh axis runs over, the one named last changes fastest.
Arguments:
- piece_tokens: bfloat16 [3072, 4096], P('kv'), may hold values from -6 to 6
- step_tokens: bfloat16 [32, 4096], P('kv'), may hold values from -6 to 6
- in_gain: float32 [4096], replicated, may hold values from 0.1 to 1.9
- w_query: bfloat16 [4096, 8, 2, 128], P(None, 'tp'), may hold values from -0.09375 to 0.09375
- w_key: bfloat16 [4096, 8, 2, 128], P(None, 'tp'), may hold values from -0.15625 to 0.15625
- w_value: bfloat16 [4096, 8, 256], P(None, 'tp'), may hold values from -0.09375 to 0.09375
- w_out: bfloat16 [8, 256, 4096], P('tp'), may hold values from -0.125 to 0.125
- mix_ratio: float32 [8], P('tp'), may hold values from 0.3 to 0.8
- out_gain: float32 [256], replicated, may hold values from 0.1 to 1.9
- prompt_keys: bfloat16 [65536, 8, 2, 128], P('kv', 'tp'), may hold values from -630 to 630
- prompt_values: bfloat16 [65536, 8, 256], P('kv', 'tp'), may hold values from -6 to 6
- step_cache_keys: bfloat16 [32, 4096, 8, 2, 128], P(None, 'kv', 'tp'), may hold values from -630 to 630
- step_cache_values: bfloat16 [32, 4096, 8, 256], P(None, 'kv', 'tp'), may hold values from -6 to 6
- prompt_len: int32 [1], replicated, may hold values from 64512 to 65536
- step_lens: int32 [32], replicated, may hold values from 4032 to 4096
Outputs:
- piece_out: bfloat16 [3072, 4096], P('kv', 'tp')
- step_out: bfloat16 [32, 4096], P('kv', 'tp')
- piece_keys: bfloat16 [3072, 8, 2, 128], P('kv', 'tp')
- piece_values: bfloat16 [3072, 8, 256], P('kv', 'tp')
- step_keys: bfloat16 [32, 8, 2, 128], P('kv', 'tp')
- step_values: bfloat16 [32, 8, 256], P('kv', 'tp')
The draws below stay inside these ranges and needn't reach their ends.
Inputs may be any that keep to these rules, and one draw needn't show every extreme that they name: `prompt_len`: the piece's tokens follow these cached positions. `step_lens`: each decoding token follows its sequence's cached positions.
All inputs are finite; a program needn't handle non-finite values.
Results may differ from the reference program's by a relative error of at most 0.015.
Values may be sent and summed in bfloat16 or wider, within the bound.
A program may use at most 128 MiB of HBM per device.

```python
import jax
import jax.numpy as jnp
from jax import lax

D = 4096
HEADS = 8
DH = 128
DV = 256
PIECE_DEV = 96
PCAP_DEV = 2048
DEC_DEV = 1
DCAP_DEV = 128
PIECE = 3072
PCAP = 65536
SEQS = 32
DEC_LEN = 4096
N_KV = 32
N_TP = 8


KEY_SCALE = 1.75


def base_keys(key, shape):
    return jnp.clip(jax.random.normal(key, shape, jnp.float32), -6.0, 6.0) * KEY_SCALE


def draw_prompt_keys(key, part):
    entries = base_keys(jax.random.fold_in(key, 3), (PCAP, HEADS, 2, DH))
    return entries.astype(jnp.bfloat16)


def draw_step_cache_keys(key, part):
    entries = base_keys(jax.random.fold_in(key, 7), (SEQS, DEC_LEN, HEADS, 2, DH))
    return entries.astype(jnp.bfloat16)


def touch_ends(array, own_key, smallest, top_value):
    longest = array.shape.index(max(array.shape))
    spots = []
    for shift in (0, 1):
        where = [jax.random.randint(jax.random.fold_in(own_key, axis), (), 0, length) for axis, length in enumerate(array.shape)]
        where[longest] = (where[longest] + shift) % array.shape[longest]
        spots.append(tuple(where))
    return array.at[spots[0]].set(smallest).at[spots[1]].set(top_value)


def block_levels(own_key, extent, pieces, low, high):
    gain = 1.0
    for dim, blocks in pieces:
        steps = jax.random.uniform(jax.random.fold_in(jax.random.fold_in(own_key, 6), dim), (blocks,), jnp.float32, low / len(pieces), high / len(pieces))
        gain = gain * jnp.repeat(jnp.exp(steps), extent[dim] // blocks).reshape((-1,) + (1,) * (len(extent) - 1 - dim))
    return gain


def noise(stream_key, dims, spread, limit, cuts=(), kind=jnp.bfloat16):
    values = spread * jax.random.normal(stream_key, dims, jnp.float32)
    if cuts:
        values = values * block_levels(stream_key, dims, cuts, -0.22, 0.18)
    return jnp.clip(values, -limit, limit).astype(kind)


def setup_inputs(seed: int = 0) -> dict:
    key_of = jax.random.split(jax.random.key(seed), 16)
    return {
        "piece_tokens": noise(key_of[0], (PIECE, D), 1.0, 6.0, ((0, 32),)),
        "step_tokens": noise(key_of[1], (SEQS, D), 1.0, 6.0, ((0, 32),)),
        "in_gain": jnp.clip(1.0 + 0.18 * jax.random.normal(key_of[2], (D,), jnp.float32), 0.1, 1.9),
        "w_query": noise(key_of[3], (D, HEADS, 2, DH), D ** -0.5, 0.09375, ((1, 8),)),
        "w_key": noise(key_of[4], (D, HEADS, 2, DH), (D // 3) ** -0.5, 0.15625, ((1, 8),)),
        "w_value": noise(key_of[5], (D, HEADS, DV), D ** -0.5, 0.09375, ((1, 8),)),
        "w_out": noise(key_of[6], (HEADS, DV, D), (HEADS * DV) ** -0.5, 0.125, ((0, 8),)),
        "mix_ratio": jnp.clip(0.3 + 0.5 * jax.random.uniform(key_of[7], (HEADS,), jnp.float32) ** block_levels(key_of[7], (HEADS,), ((0, 8),), -0.2, 0.2), 0.3, 0.8),
        "out_gain": jnp.clip(1.0 + 0.18 * jax.random.normal(key_of[8], (DV,), jnp.float32), 0.1, 1.9),
        "prompt_keys": draw_prompt_keys(jax.random.fold_in(key_of[15], 71), 0),
        "prompt_values": noise(key_of[10], (PCAP, HEADS, DV), 1.0, 6.0, ((0, 32), (1, 8))),
        "step_cache_keys": draw_step_cache_keys(jax.random.fold_in(key_of[15], 71), 0),
        "step_cache_values": noise(key_of[12], (SEQS, DEC_LEN, HEADS, DV), 1.0, 6.0, ((1, 32), (2, 8))),
        "prompt_len": jax.random.randint(key_of[13], (1,), PCAP - PCAP_DEV // 2, PCAP + 1).astype(jnp.int32),
        "step_lens": touch_ends(jax.random.randint(key_of[14], (SEQS,), DEC_LEN - DCAP_DEV // 2, DEC_LEN + 1), jax.random.fold_in(key_of[14], 1), DEC_LEN - DCAP_DEV // 2, DEC_LEN).astype(jnp.int32),
    }


EPS = 1e-06
OUT_SCALE = 0.8

def norm_rows(tokens, in_gain):
    floats = tokens.astype(jnp.float32)
    inv_rms = lax.rsqrt(lax.optimization_barrier(jnp.mean(floats * floats, axis=-1, keepdims=True)) + EPS)
    return (floats * inv_rms * in_gain.astype(jnp.float32)).astype(jnp.bfloat16)

def project(normed, weight):
    flat_weight = weight.reshape(weight.shape[0], -1)
    product = jnp.dot(normed, flat_weight, preferred_element_type=jnp.float32)
    rounded = lax.optimization_barrier(product.astype(jnp.bfloat16))
    return rounded.reshape((normed.shape[0],) + weight.shape[1:])

def head_partial(queries, key_rows, value_rows, visible):
    scores = jnp.einsum('qcd,kcd->cqk', queries.astype(jnp.float32), key_rows.astype(jnp.float32))
    scores = scores * queries.shape[-1] ** (-0.5)
    scores = jnp.where(visible[None], scores, -jnp.inf)
    maxima = lax.optimization_barrier(jnp.max(scores, axis=-1))
    weights = jnp.exp(scores - maxima[..., None])
    totals = lax.optimization_barrier(jnp.sum(weights, axis=-1))
    rounded = lax.optimization_barrier(weights.astype(jnp.bfloat16))
    summed = jnp.einsum('cqk,kv->qcv', rounded.astype(jnp.float32), value_rows.astype(jnp.float32))
    summed = lax.optimization_barrier(summed.astype(jnp.bfloat16))
    return (summed, jnp.transpose(maxima), jnp.transpose(totals))

def fold_group(running, summed, maxima, totals):
    row_best, norm_sum, value_sum = running
    new_best = jnp.maximum(row_best, maxima)
    old_scale = jnp.exp(row_best - new_best)
    new_scale = jnp.exp(maxima - new_best)
    return (new_best, norm_sum * old_scale + totals * new_scale, value_sum * old_scale[..., None] + summed.astype(jnp.float32) * new_scale[..., None])

def finish(norm_sum, value_sum, mix_ratio, out_gain):
    attended = value_sum / norm_sum[..., None]
    mixed = attended[:, :, 0] - mix_ratio[None, :, None] * attended[:, :, 1]
    inv_rms = lax.rsqrt(lax.optimization_barrier(jnp.mean(mixed * mixed, axis=-1, keepdims=True)) + EPS)
    return (mixed * inv_rms * out_gain[None, None, :] * OUT_SCALE).astype(jnp.bfloat16)

def empty_state(row_count):
    return (jnp.full((row_count, HEADS, 2), -jnp.inf, jnp.float32), jnp.zeros((row_count, HEADS, 2), jnp.float32), jnp.zeros((row_count, HEADS, 2, DV), jnp.float32))

def reference(piece_tokens, step_tokens, in_gain, w_query, w_key, w_value, w_out, mix_ratio, out_gain, prompt_keys, prompt_values, step_cache_keys, step_cache_values, prompt_len, step_lens):
    all_rows = jnp.concatenate([piece_tokens, step_tokens], axis=0)
    normed = norm_rows(all_rows, in_gain)
    queries = project(normed, w_query)
    key_rows = project(normed, w_key)
    value_rows = project(normed, w_value)
    piece_q = queries[:PIECE]
    step_q = queries[PIECE:]
    piece_k = key_rows[:PIECE]
    step_k = key_rows[PIECE:]
    piece_v = value_rows[:PIECE]
    step_v = value_rows[PIECE:]
    row_place = jnp.arange(PIECE, dtype=jnp.int32)
    seq_place = jnp.arange(SEQS, dtype=jnp.int32)

    def piece_group(running, group_id):
        cache_k = lax.dynamic_slice_in_dim(prompt_keys, group_id * PCAP_DEV, PCAP_DEV, 0)
        cache_v = lax.dynamic_slice_in_dim(prompt_values, group_id * PCAP_DEV, PCAP_DEV, 0)
        fresh_k = lax.dynamic_slice_in_dim(piece_k, group_id * PIECE_DEV, PIECE_DEV, 0)
        fresh_v = lax.dynamic_slice_in_dim(piece_v, group_id * PIECE_DEV, PIECE_DEV, 0)
        all_k = jnp.concatenate([cache_k, fresh_k], axis=0)
        all_v = jnp.concatenate([cache_v, fresh_v], axis=0)
        cache_place = group_id * PCAP_DEV + jnp.arange(PCAP_DEV, dtype=jnp.int32)
        fresh_place = group_id * PIECE_DEV + jnp.arange(PIECE_DEV, dtype=jnp.int32)
        visible = jnp.concatenate([jnp.broadcast_to((cache_place < prompt_len[0])[None, :], (PIECE, PCAP_DEV)), fresh_place[None, :] <= row_place[:, None]], axis=1)

        def one_head(operands):
            return head_partial(operands[0], operands[1], operands[2], visible)
        summed, maxima, totals = lax.map(one_head, (jnp.moveaxis(piece_q, 1, 0), jnp.moveaxis(all_k, 1, 0), jnp.moveaxis(all_v, 1, 0)))
        return (fold_group(running, jnp.moveaxis(summed, 0, 1), jnp.moveaxis(maxima, 0, 1), jnp.moveaxis(totals, 0, 1)), None)
    piece_state = lax.scan(piece_group, empty_state(PIECE), jnp.arange(N_KV, dtype=jnp.int32))[0]

    def step_group(running, group_id):
        cache_k = lax.dynamic_slice_in_dim(step_cache_keys, group_id * DCAP_DEV, DCAP_DEV, 1)
        cache_v = lax.dynamic_slice_in_dim(step_cache_values, group_id * DCAP_DEV, DCAP_DEV, 1)
        all_k = jnp.concatenate([cache_k, step_k[:, None]], axis=1)
        all_v = jnp.concatenate([cache_v, step_v[:, None]], axis=1)
        cache_place = group_id * DCAP_DEV + jnp.arange(DCAP_DEV, dtype=jnp.int32)
        visible = jnp.concatenate([cache_place[None, :] < step_lens[:, None], (seq_place // DEC_DEV == group_id)[:, None]], axis=1)
        scores = jnp.einsum('bhcd,bkhcd->bhck', step_q.astype(jnp.float32), all_k.astype(jnp.float32))
        scores = scores * DH ** (-0.5)
        scores = jnp.where(visible[:, None, None, :], scores, -jnp.inf)
        maxima = lax.optimization_barrier(jnp.max(scores, axis=-1))
        weights = jnp.exp(scores - maxima[..., None])
        totals = lax.optimization_barrier(jnp.sum(weights, axis=-1))
        rounded = lax.optimization_barrier(weights.astype(jnp.bfloat16))
        summed = jnp.einsum('bhck,bkhv->bhcv', rounded.astype(jnp.float32), all_v.astype(jnp.float32))
        summed = lax.optimization_barrier(summed.astype(jnp.bfloat16))
        return (fold_group(running, summed, maxima, totals), None)
    step_state = lax.scan(step_group, empty_state(SEQS), jnp.arange(N_KV, dtype=jnp.int32))[0]
    headout = jnp.concatenate([finish(piece_state[1], piece_state[2], mix_ratio, out_gain), finish(step_state[1], step_state[2], mix_ratio, out_gain)], axis=0)
    total_rows = PIECE + SEQS
    per_group = HEADS // N_TP
    grouped = jnp.moveaxis(headout.reshape(total_rows, N_TP, per_group * DV), 1, 0)
    weights = w_out.reshape(N_TP, per_group * DV, D)

    def group_term(operands):
        return jnp.dot(operands[0], operands[1], preferred_element_type=jnp.float32).astype(jnp.bfloat16)
    terms = lax.optimization_barrier(lax.map(group_term, (grouped, weights)))
    mixed = lax.optimization_barrier(jnp.sum(terms.astype(jnp.float32), axis=0)).astype(jnp.bfloat16)
    return (mixed[:PIECE], mixed[PIECE:], piece_k, piece_v, step_k, step_v)
```

```python
import functools
import math

import jax
import jax.numpy as jnp
from jax import lax
from jax.experimental import pallas as pl
from jax.experimental.pallas import tpu as pltpu
from jax.sharding import PartitionSpec as P

EPS = 1e-06
OUT_SCALE = 0.8
NZ, NY, NKV = 8, 4, 32
ROWS = 96
CHUNKS = 3
R = ROWS // CHUNKS
RD = 16
TILE = NZ * R
TILED = NZ * RD
CACHE = 2048
KEYS = CACHE + 128
SEQC = 128
DH, DV = 128, 256
PADDED = ROWS + RD
EXPC = DH ** (-0.5) * math.log2(math.e)
STAT_Z = (1, 3, 5, 7)
F32, BF16 = jnp.float32, jnp.bfloat16
NT = (((1,), (1,)), ((), ()))


def attend(
    q_own, k_own, v_own, kp_hbm, vp_hbm, kd_hbm, vd_hbm, gain_ref, plen, slens, mix,
    out_ref,
    kbuf, vnat, vt, kd, vdn, vtd, ksd, vse, qall, qd, bias, sbuf, pbuf, oacc, oaccd,
    stat, srecv, ressend, res, comb, combd, rh, rhd, rf, rfd, acc, accb, accbd, rz, rzd, mixed,
    load_sem, zs, zr, ys, yr, hs, hr, ss, sr, rs, rr, xs, xr, fs, fr, ws, wr,
):
    me = lax.axis_index("kv")
    z = me // NY
    y = me % NY
    yp, ym, y2 = (y + 1) % NY, (y + 3) % NY, (y + 2) % NY

    def at_kv(index):
        return {"kv": index}

    def rcopy(src, dst, s_sem, r_sem, target):
        return pltpu.make_async_remote_copy(
            src_ref=src, dst_ref=dst, send_sem=s_sem, recv_sem=r_sem,
            device_id=at_kv(target), device_id_type=pl.DeviceIdType.MESH,
        )

    def rows_of(j):
        return R if j < CHUNKS else RD

    def qtile(j, yy):
        return qall.at[j * NY + yy] if j < CHUNKS else qd.at[yy]

    def ctile(j, yy):
        return comb.at[j * NY + yy] if j < CHUNKS else combd.at[yy]

    def zblock(view, zz, n):
        return view.at[pl.ds(pl.multiple_of(zz * n, n), n), :]

    barrier = pltpu.get_barrier_semaphore()

    @pl.loop(1, NKV)
    def _(d):
        pl.semaphore_signal(
            barrier, inc=1, device_id=at_kv((me + d) % NKV),
            device_id_type=pl.DeviceIdType.MESH,
        )

    loads = [
        pltpu.make_async_copy(kp_hbm, kbuf.at[pl.ds(0, CACHE), :], load_sem.at[0]),
        pltpu.make_async_copy(vp_hbm, vnat, load_sem.at[1]),
        pltpu.make_async_copy(kd_hbm, kd, load_sem.at[2]),
        pltpu.make_async_copy(vd_hbm, vdn, load_sem.at[3]),
    ]
    for load in loads:
        load.start()

    for j in range(4):
        n = rows_of(j)
        lo = j * R if j < CHUNKS else ROWS
        mine = qtile(j, y)
        mine[pl.ds(pl.multiple_of(z * n, n), n), :] = q_own[lo : lo + n, :]

    pl.semaphore_wait(barrier, NKV - 1)

    def z_copy(j, d):
        n = rows_of(j)
        zt = (z + d) % NZ
        block = zblock(qtile(j, y), z, n)
        return rcopy(block, block, zs.at[j, d], zr.at[j, d], zt * NY + y)

    for j in range(4):
        for d in (1, 7, 2, 6, 3, 5, 4):
            z_copy(j, d).start()

    kbuf[CACHE : CACHE + ROWS, :] = k_own[:ROWS, :]
    kbuf[CACHE + ROWS :, :] = jnp.zeros((KEYS - CACHE - ROWS, 2 * DH), BF16)
    ksd[:RD, :] = k_own[ROWS:, :]
    ksd[RD:, :] = jnp.zeros((SEQC - RD, 2 * DH), BF16)
    tail = jnp.concatenate([v_own[:ROWS, :], jnp.zeros((128 - ROWS, DV), BF16)], axis=0)
    vt[:, CACHE:] = tail.T
    tail = jnp.concatenate([v_own[ROWS:, :], jnp.zeros((128 - RD, DV), BF16)], axis=0)
    vse[...] = tail.T
    half = CACHE // 2
    place = me * CACHE + half + lax.broadcasted_iota(jnp.int32, (half, 128), 0)
    bias[...] = jnp.where(place < plen[0], 0.0, -jnp.inf).astype(F32)
    loads[0].wait()
    loads[1].wait()
    for b in range(CACHE // 256):
        vt[:, b * 256 : (b + 1) * 256] = vnat[b * 256 : (b + 1) * 256, :].T

    def z_wait_y_send(j):
        n = rows_of(j)
        for d in range(1, NZ):
            zf = (z + NZ - d) % NZ
            block = zblock(qtile(j, y), zf, n)
            rcopy(block, block, zs.at[j, d], zr.at[j, d], zf * NY + y).wait_recv()
        y_copy(j, 0).start()
        y_copy(j, 1).start()

    def y_copy(j, side):
        tile = qtile(j, y)
        return rcopy(tile, tile, ys.at[j, side], yr.at[j, side], z * NY + (yp if side == 0 else ym))

    def half_of(view, j, side):
        h = NZ * rows_of(j) // 2
        return view.at[pl.ds(side * h, h), :]

    def h_copy(j, side):
        part = half_of(qtile(j, ym if side == 0 else yp), j, side)
        return rcopy(part, part, hs.at[j, side], hr.at[j, side], z * NY + (yp if side == 0 else ym))

    def y_wait_fwd(j):
        for side in (0, 1):
            tile = qtile(j, ym if side == 0 else yp)
            rcopy(tile, tile, ys.at[j, side], yr.at[j, side], z * NY + y2).wait_recv()
            h_copy(j, side).start()

    def h_wait(j):
        for side in (0, 1):
            part = half_of(qtile(j, y2), j, side)
            rcopy(part, part, hs.at[j, side], hr.at[j, side], z * NY + y2).wait_recv()

    KB = [(b * 256, 256) for b in range(CACHE // 256)] + [(CACHE, 128)]

    @pl.loop(0, CHUNKS * NY)
    def _(t):
        for step, work in (
            (0, lambda: z_wait_y_send(0)),
            (1, lambda: z_wait_y_send(1)),
            (1, lambda: y_wait_fwd(0)),
            (2, lambda: z_wait_y_send(2)),
            (3, lambda: h_wait(0)),
            (3, lambda: z_wait_y_send(3)),
            (4, lambda: y_wait_fwd(1)),
            (5, lambda: y_wait_fwd(2)),
            (6, lambda: y_wait_fwd(3)),
            (7, lambda: h_wait(1)),
            (11, lambda: h_wait(2)),
        ):
            pl.when(t == step)(work)

        j = t // NY
        i = t % NY
        yy = (y + jnp.where(i == 2, 3, jnp.where(i == 3, 2, i))) % NY
        tt = j * NY + yy
        lane = lax.broadcasted_iota(jnp.int32, (128, TILE), 1)
        row = lax.broadcasted_iota(jnp.int32, (128, TILE), 0)
        row_place = ((lane // R) * NY + yy) * ROWS + R * j + lane % R
        fresh_ok = (row < ROWS) & (me * ROWS + row <= row_place)
        for c in range(2):
            cols = slice(c * DH, (c + 1) * DH)
            q = qall[tt, :, cols]
            top = jnp.full((8, TILE), -jnp.inf, F32)
            for at, size in KB:
                s = lax.dot_general(kbuf[at : at + size, cols], q, NT, preferred_element_type=F32)
                if at == CACHE:
                    s = jnp.where(fresh_ok, s, -jnp.inf)
                elif at >= half:
                    b = bias[at - half : at - half + size, :]
                    s = s + jnp.concatenate([b, b], axis=1)
                sbuf[c, at : at + size, :] = s
                top = jnp.maximum(top, jnp.max(s.reshape(size // 8, 8, TILE), axis=0))
            m = jnp.max(top, axis=0, keepdims=True)
            total = jnp.zeros((8, TILE), F32)
            for at, size in KB:
                w = jnp.exp2((sbuf[c, at : at + size, :] - m) * EXPC)
                total = total + jnp.sum(w.reshape(size // 8, 8, TILE), axis=0)
                pbuf[c, at : at + size, :] = w.astype(BF16)
            total = jnp.sum(total, axis=0, keepdims=True)
            oacc[tt, c] = jnp.dot(vt[...], pbuf[c], preferred_element_type=F32)
            for hh in range(2):
                stat[tt, 2 * c + hh : 2 * c + hh + 1, :] = m[:, hh * 128 : (hh + 1) * 128]
                stat[tt, 4 + 2 * c + hh : 5 + 2 * c + hh, :] = total[:, hh * 128 : (hh + 1) * 128]

    loads[2].wait()
    loads[3].wait()
    h_wait(3)

    @pl.loop(0, NY)
    def _(yy):
        q2 = qd[yy]
        lane = lax.broadcasted_iota(jnp.int32, (SEQC, TILED), 1)
        row = lax.broadcasted_iota(jnp.int32, (SEQC, TILED), 0)
        own = (lane // RD == jnp.where(yy == y, z, NZ)) & (row == 0)
        for zz in range(NZ):
            vtd[:, zz * SEQC : (zz + 1) * SEQC] = vdn[zz * NY + yy].T
        stat[CHUNKS * NY + yy] = jnp.where(lax.broadcasted_iota(jnp.int32, (8, 128), 0) < 4, 0.0, 1.0)
        for c in range(2):
            cols = slice(c * DH, (c + 1) * DH)
            q = q2[:, cols]
            parts = []
            top = jnp.full((8, TILED), -jnp.inf, F32)
            for zz in range(NZ + 1):
                if zz < NZ:
                    k = kd[zz * NY + yy, :, cols]
                    ok = (lane // RD == zz) & (me * SEQC + row < slens[zz * NY + yy])
                else:
                    k = ksd[:, cols]
                    ok = own
                s = lax.dot_general(k, q, NT, preferred_element_type=F32)
                s = jnp.where(ok, s, -jnp.inf)
                parts.append(s)
                top = jnp.maximum(top, jnp.max(s.reshape(SEQC // 8, 8, TILED), axis=0))
            m = jnp.max(top, axis=0, keepdims=True)
            total = jnp.zeros((8, TILED), F32)
            out = jnp.zeros((DV, TILED), F32)
            for zz in range(NZ + 1):
                w = jnp.exp2((parts[zz] - m) * EXPC)
                total = total + jnp.sum(w.reshape(SEQC // 8, 8, TILED), axis=0)
                v = vtd[:, zz * SEQC : (zz + 1) * SEQC] if zz < NZ else vse[...]
                out = out + jnp.dot(v, w.astype(BF16), preferred_element_type=F32)
            oaccd[yy, c] = out
            stat[CHUNKS * NY + yy, 2 * c : 2 * c + 1, :] = m
            stat[CHUNKS * NY + yy, 4 + 2 * c : 5 + 2 * c, :] = jnp.sum(total, axis=0, keepdims=True)

    def s_copy(j, yt):
        return rcopy(
            stat.at[j * NY + yt], srecv.at[j, me], ss.at[j, yt], sr.at[j, me], STAT_Z[j] * NY + yt
        )

    def stats_send(j):
        for yt in range(NY):
            target = STAT_Z[j] * NY + yt

            @pl.when(target != me)
            def _():
                s_copy(j, yt).start()

            @pl.when(target == me)
            def _():
                srecv[j, me] = stat[j * NY + yt]

    def r_copy(j, target):
        return rcopy(ressend.at[j], res.at[j * NY + y], rs.at[j, target], rr.at[j, y], target)

    def stats_own(j):
        @pl.when(z == STAT_Z[j])
        def _():
            @pl.loop(1, NKV)
            def _(d):
                src = (me + d) % NKV
                rcopy(stat.at[0], srecv.at[j, src], ss.at[j, 0], sr.at[j, src], src).wait_recv()

            every = srecv[j]
            best = jnp.max(every[:, 0:4, :], axis=0)
            norm = jnp.sum(every[:, 4:8, :] * jnp.exp2((every[:, 0:4, :] - best[None]) * EXPC), axis=0)
            both = jnp.concatenate([best, 1.0 / norm], axis=0)
            ressend[j] = both
            res[j * NY + y] = both

            @pl.loop(1, NKV)
            def _(d):
                r_copy(j, (me + d) % NKV).start()

    def stats_wait(j):
        for yt in range(NY):
            owner = STAT_Z[j] * NY + yt

            @pl.when(owner != me)
            def _():
                rcopy(ressend.at[j], res.at[j * NY + yt], rs.at[j, owner], rr.at[j, yt], owner).wait_recv()

    for j in range(4):
        stats_send(j)
    for j in range(4):
        stats_own(j)

    def combine(j):
        wide = 2 if j < CHUNKS else 1

        @pl.loop(0, NY)
        def _(yy):
            tt = j * NY + yy
            factors = []
            for c in range(2):
                pick = lambda ref, lo: jnp.concatenate(
                    [ref[tt, lo + 2 * c + hh : lo + 2 * c + hh + 1, :] for hh in range(wide)], axis=1
                )
                factors.append(jnp.exp2((pick(stat, 0) - pick(res, 0)) * EXPC) * pick(res, 4))
            values = oacc if j < CHUNKS else oaccd
            at = tt if j < CHUNKS else yy
            both = values[at, 0] * factors[0] - values[at, 1] * (factors[1] * mix[0])
            ctile(j, yy)[...] = both.T.astype(BF16)

    def x_copy(j, side):
        part = half_of(ctile(j, y2), j, side)
        land = rh.at[j, side] if j < CHUNKS else rhd.at[side]
        return rcopy(part, land, xs.at[j, side], xr.at[j, side], z * NY + (yp if side == 0 else ym))

    def f_copy(j, side):
        tile = ctile(j, yp if side == 0 else ym)
        land = rf.at[j, side] if j < CHUNKS else rfd.at[side]
        return rcopy(tile, land, fs.at[j, side], fr.at[j, side], z * NY + (yp if side == 0 else ym))

    def rs_second(j):
        h = NZ * rows_of(j) // 2
        for side in (0, 1):
            x_copy(j, side).wait_recv()
            land = rh[j, side] if j < CHUNKS else rhd[side]
            part = half_of(ctile(j, yp if side == 0 else ym), j, side)
            part[...] = (part[...].astype(F32) + land.astype(F32)).astype(BF16)
            f_copy(j, side).start()

    def wire_block(j, zz):
        n = rows_of(j)
        return zblock(accb.at[j] if j < CHUNKS else accbd, zz, n)

    def w_copy(j, d):
        zt = (z + d) % NZ
        land = rz.at[j, d] if j < CHUNKS else rzd.at[d]
        return rcopy(wire_block(j, zt), land, ws.at[j, d], wr.at[j, d], zt * NY + y)

    def rs_third(j):
        n = rows_of(j)
        for side in (0, 1):
            f_copy(j, side).wait_recv()
        if j < CHUNKS:
            total = comb[j * NY + y].astype(F32) + rf[j, 0].astype(F32) + rf[j, 1].astype(F32)
            accb[j] = total.astype(BF16)
        else:
            total = combd[y].astype(F32) + rfd[0].astype(F32) + rfd[1].astype(F32)
            accbd[...] = total.astype(BF16)
        acc[j, : NZ * n, :] = total
        for d in (4, 3, 5, 2, 6, 1, 7):
            w_copy(j, d).start()

    def rs_last(j):
        n = rows_of(j)
        lo = j * R if j < CHUNKS else ROWS
        total = acc[j, pl.ds(pl.multiple_of(z * n, n), n), :]
        for d in range(1, NZ):
            w_copy(j, d).wait_recv()
            total = total + (rz[j, d] if j < CHUNKS else rzd[d]).astype(F32)
        mixed[lo : lo + n, :] = total

    for j in range(4):
        stats_wait(j)
        combine(j)
        for side in (0, 1):
            x_copy(j, side).start()
    for j in range(4):
        rs_second(j)
    for j in range(4):
        rs_third(j)
    for j in range(4):
        rs_last(j)

    total = mixed[...]
    inv_rms = lax.rsqrt(jnp.mean(total * total, axis=-1, keepdims=True) + EPS)
    out_ref[...] = (total * inv_rms * gain_ref[...] * OUT_SCALE).astype(BF16)

    for j in range(4):
        for d in range(1, NZ):
            z_copy(j, d).wait_send()
            w_copy(j, d).wait_send()
        for side in (0, 1):
            y_copy(j, side).wait_send()
            h_copy(j, side).wait_send()
            x_copy(j, side).wait_send()
            f_copy(j, side).wait_send()
        for yt in range(NY):

            @pl.when(STAT_Z[j] * NY + yt != me)
            def _():
                s_copy(j, yt).wait_send()

        @pl.when(z == STAT_Z[j])
        def _():
            @pl.loop(1, NKV)
            def _(d):
                r_copy(j, (me + d) % NKV).wait_send()


def attention(q, k, v, kp, vp, kd, vd, gain, prompt_len, step_lens, mix):
    vmem = pl.BlockSpec(memory_space=pltpu.VMEM)
    anyw = pl.BlockSpec(memory_space=pl.ANY)
    smem = pl.BlockSpec(memory_space=pltpu.SMEM)
    dma = pltpu.SemaphoreType.DMA
    V = pltpu.VMEM
    nt = CHUNKS * NY
    return pl.pallas_call(
        attend,
        out_shape=jax.ShapeDtypeStruct((PADDED, DV), BF16),
        in_specs=[vmem, vmem, vmem, anyw, anyw, anyw, anyw, vmem, smem, smem, smem],
        out_specs=vmem,
        scratch_shapes=[
            V((KEYS, 2 * DH), BF16),
            V((CACHE, DV), BF16),
            V((DV, KEYS), BF16),
            V((NKV, SEQC, 2 * DH), BF16),
            V((NKV, SEQC, DV), BF16),
            V((DV, NZ * SEQC), BF16),
            V((SEQC, 2 * DH), BF16),
            V((DV, SEQC), BF16),
            V((nt, TILE, 2 * DH), BF16),
            V((NY, TILED, 2 * DH), BF16),
            V((CACHE // 2, 128), F32),
            V((2, KEYS, TILE), F32),
            V((2, KEYS, TILE), BF16),
            V((nt, 2, DV, TILE), F32),
            V((NY, 2, DV, TILED), F32),
            V((nt + NY, 8, 128), F32),
            V((4, NKV, 8, 128), F32),
            V((4, 8, 128), F32),
            V((nt + NY, 8, 128), F32),
            V((nt, TILE, DV), BF16),
            V((NY, TILED, DV), BF16),
            V((CHUNKS, 2, TILE // 2, DV), BF16),
            V((2, TILED // 2, DV), BF16),
            V((CHUNKS, 2, TILE, DV), BF16),
            V((2, TILED, DV), BF16),
            V((4, TILE, DV), F32),
            V((CHUNKS, TILE, DV), BF16),
            V((TILED, DV), BF16),
            V((CHUNKS, NZ, R, DV), BF16),
            V((NZ, RD, DV), BF16),
            V((PADDED, DV), F32),
            dma((4,)),
            dma((4, NZ)), dma((4, NZ)),
            dma((4, 2)), dma((4, 2)),
            dma((4, 2)), dma((4, 2)),
            dma((4, NY)), dma((4, NKV)),
            dma((4, NKV)), dma((4, NY)),
            dma((4, 2)), dma((4, 2)),
            dma((4, 2)), dma((4, 2)),
            dma((4, NZ)), dma((4, NZ)),
        ],
        compiler_params=pltpu.CompilerParams(
            collective_id=0, has_side_effects=True, vmem_limit_bytes=60 << 20
        ),
        name="attend",
    )(q, k, v, kp, vp, kd, vd, gain, prompt_len, step_lens, mix)


def norm_rows(tokens, in_gain):
    floats = tokens.astype(F32)
    inv_rms = lax.rsqrt(jnp.mean(floats * floats, axis=-1, keepdims=True) + EPS)
    return (floats * inv_rms * in_gain).astype(BF16)


def project(normed, weight):
    flat_weight = weight.reshape(weight.shape[0], -1)
    return jnp.dot(normed, flat_weight, preferred_element_type=F32).astype(BF16)


def summed_on_arrival(shard, axis):
    count = lax.axis_size(axis)
    blocks = jnp.moveaxis(shard.reshape(shard.shape[0], count, -1), 1, 0)
    blocks = lax.all_to_all(blocks, axis, 0, 0, tiled=True)
    return jnp.sum(blocks.astype(F32), axis=0)


def on_device(
    piece_tokens, step_tokens, in_gain, w_query, w_key, w_value, w_out, mix_ratio, out_gain,
    prompt_keys, prompt_values, step_cache_keys, step_cache_values, prompt_len, step_lens,
):
    pad = jnp.zeros((RD - 1, piece_tokens.shape[1]), BF16)
    normed = norm_rows(jnp.concatenate([piece_tokens, step_tokens, pad], axis=0), in_gain)
    q = project(normed, w_query)
    k = project(normed, w_key)
    v = project(normed, w_value)
    headout = attention(
        q, k, v,
        prompt_keys.reshape(CACHE, 2 * DH), prompt_values.reshape(CACHE, DV),
        step_cache_keys.reshape(NKV, SEQC, 2 * DH), step_cache_values.reshape(NKV, SEQC, DV),
        out_gain.reshape(1, DV), prompt_len, step_lens, mix_ratio,
    )
    head_term = jnp.dot(
        headout[: ROWS + 1], w_out.reshape(-1, w_out.shape[-1]), preferred_element_type=F32
    ).astype(BF16)
    out = summed_on_arrival(head_term, "tp").astype(BF16)
    return (
        out[:ROWS], out[ROWS:],
        k[:ROWS].reshape(ROWS, 1, 2, DH), v[:ROWS].reshape(ROWS, 1, DV),
        k[ROWS : ROWS + 1].reshape(1, 1, 2, DH), v[ROWS : ROWS + 1].reshape(1, 1, DV),
    )


def solution(mesh):
    in_specs = (
        P("kv", None),
        P("kv", None),
        P(),
        P(None, "tp", None, None),
        P(None, "tp", None, None),
        P(None, "tp", None),
        P("tp", None, None),
        P("tp"),
        P(),
        P("kv", "tp", None, None),
        P("kv", "tp", None),
        P(None, "kv", "tp", None, None),
        P(None, "kv", "tp", None),
        P(),
        P(),
    )
    out_specs = (
        P("kv", "tp"),
        P("kv", "tp"),
        P("kv", "tp", None, None),
        P("kv", "tp", None),
        P("kv", "tp", None, None),
        P("kv", "tp", None),
    )
    return jax.shard_map(
        on_device, mesh=mesh, in_specs=in_specs, out_specs=out_specs, check_vma=False
    )
```

```python
import functools
import math

import jax
import jax.numpy as jnp
from jax import lax
from jax.experimental import pallas as pl
from jax.experimental.pallas import tpu as pltpu
from jax.sharding import PartitionSpec as P

EPS = 1e-06
OUT_SCALE = 0.8
NZ, NY, NKV, NX = 8, 4, 32, 4
D, OUTB = 4096, 512
ROWS = 96
CHUNKS = 3
R = ROWS // CHUNKS
RD = 16
TILE = NZ * R
TILED = NZ * RD
CACHE = 2048
KEYS = CACHE + 128
SEQC = 128
DH, DV = 128, 256
PADDED = ROWS + RD
EXPC = DH ** (-0.5) * math.log2(math.e)
STAT_Z = (1, 4, 7)
F32, BF16 = jnp.float32, jnp.bfloat16
NT = (((1,), (1,)), ((), ()))


def attend(
    q_own, k_own, normed, wv_hbm, kp_hbm, vp_hbm, kd_hbm, vd_hbm, wo_hbm, gain_ref, plen, slens, mix,
    piece_ref, step_ref, pv_ref, sv_ref,
    wv, wo, kraw, kfloat, kbuf, vnat, vt, kd, vdn, vtd, ksd, vse, qall, qd, bias, sbuf, pbuf, oacc,
    stat, srecv, ressend, res, dsend, drecv, comb, rh, rf, acc, accb, rz, mixed,
    term, tsum, pr, th, tf,
    load_sem, zs, zr, ys, yr, hs, hr, ss, sr, rs, rr, xs, xr, fs, fr, ws, wr, ds, dr,
    ps, ps_r, ts, tr, us, ur,
):
    me = lax.axis_index("kv")
    tp = lax.axis_index("tp")
    z = me // NY
    y = me % NY
    yp, ym, y2 = (y + 1) % NY, (y + 3) % NY, (y + 2) % NY
    x = tp // 2
    core = tp % 2
    xp, xm, x2 = (x + 1) % NX, (x + 3) % NX, (x + 2) % NX

    def at_kv(index):
        return {"kv": index}

    def rcopy(src, dst, s_sem, r_sem, target):
        return pltpu.make_async_remote_copy(
            src_ref=src, dst_ref=dst, send_sem=s_sem, recv_sem=r_sem,
            device_id=at_kv(target), device_id_type=pl.DeviceIdType.MESH,
        )

    def tcopy(src, dst, s_sem, r_sem, tx, tc):
        return pltpu.make_async_remote_copy(
            src_ref=src, dst_ref=dst, send_sem=s_sem, recv_sem=r_sem,
            device_id={"tp": tx * 2 + tc}, device_id_type=pl.DeviceIdType.MESH,
        )

    def rows_of(j):
        return R if j < CHUNKS else RD

    def qtile(j, yy):
        return qall.at[j * NY + yy] if j < CHUNKS else qd.at[yy]

    def ctile(j, yy):
        return comb.at[j * NY + yy]

    def zblock(view, zz, n):
        return view.at[pl.ds(pl.multiple_of(zz * n, n), n), :]

    barrier = pltpu.get_barrier_semaphore()

    @pl.loop(1, NKV)
    def _(d):
        pl.semaphore_signal(
            barrier, inc=1, device_id=at_kv((me + d) % NKV),
            device_id_type=pl.DeviceIdType.MESH,
        )

    for tx, tc in ((x, 1 - core), (xp, core), (xm, core)):
        pl.semaphore_signal(
            barrier, inc=1, device_id={"tp": tx * 2 + tc}, device_id_type=pl.DeviceIdType.MESH
        )

    loads = [
        pltpu.make_async_copy(wv_hbm, wv, load_sem.at[0]),
        pltpu.make_async_copy(kp_hbm, kraw.at[pl.ds(0, 2 * CACHE), :], load_sem.at[1]),
        pltpu.make_async_copy(vp_hbm, vnat, load_sem.at[2]),
        pltpu.make_async_copy(kd_hbm, kraw.at[pl.ds(2 * CACHE, 2 * NKV * SEQC), :], load_sem.at[3]),
        pltpu.make_async_copy(vd_hbm, vdn, load_sem.at[4]),
        pltpu.make_async_copy(wo_hbm, wo, load_sem.at[5]),
    ]
    for load in loads:
        load.start()

    for j in range(4):
        n = rows_of(j)
        lo = j * R if j < CHUNKS else ROWS
        mine = qtile(j, y)
        mine[pl.ds(pl.multiple_of(z * n, n), n), :] = q_own[lo : lo + n, :]

    pl.semaphore_wait(barrier, NKV - 1 + 3)

    def z_copy(j, d):
        n = rows_of(j)
        zt = (z + d) % NZ
        block = zblock(qtile(j, y), z, n)
        return rcopy(block, block, zs.at[j], zr.at[j], zt * NY + y)

    def z_all(j):
        some = qtile(j, y).at[pl.ds(0, (NZ - 1) * rows_of(j)), :]
        return rcopy(some, some, zs.at[j], zr.at[j], z * NY + yp)

    for j in range(4):
        for d in (1, 7, 2, 6, 3, 5, 4):
            z_copy(j, d).start()

    loads[0].wait()
    values = jnp.dot(normed[...], wv[...], preferred_element_type=F32).astype(BF16)
    pv_ref[...] = values[:ROWS, :]
    sv_ref[...] = values[ROWS : ROWS + 1, :]
    kbuf[CACHE : CACHE + ROWS, :] = k_own[:ROWS, :]
    kbuf[CACHE + ROWS :, :] = jnp.zeros((KEYS - CACHE - ROWS, 2 * DH), BF16)
    ksd[:RD, :] = k_own[ROWS:, :]
    ksd[RD:, :] = jnp.zeros((SEQC - RD, 2 * DH), BF16)
    tail = jnp.concatenate([values[:ROWS, :], jnp.zeros((128 - ROWS, DV), BF16)], axis=0)
    vt[:, CACHE:] = tail.T
    tail = jnp.concatenate([values[ROWS:, :], jnp.zeros((128 - RD, DV), BF16)], axis=0)
    vse[...] = tail.T
    half = CACHE // 2
    place = me * CACHE + half + lax.broadcasted_iota(jnp.int32, (half, 128), 0)
    bias[...] = jnp.where(place < plen[0], 0.0, -jnp.inf).astype(F32)
    mixed[...] = jnp.zeros((PADDED, DV), F32)
    loads[1].wait()
    loads[2].wait()

    @pl.loop(0, CACHE // 256)
    def _(b):
        kfloat[...] = kraw[pl.ds(pl.multiple_of(b * 512, 512), 512), :].astype(F32)
        rows = pl.ds(pl.multiple_of(b * 256, 256), 256)
        for c in range(2):
            kbuf[rows, c * DH : (c + 1) * DH] = kfloat[pl.ds(c, 256, 2), :].astype(BF16)

    for b in range(CACHE // 256):
        vt[:, b * 256 : (b + 1) * 256] = vnat[b * 256 : (b + 1) * 256, :].T
    loads[3].wait()

    @pl.loop(0, NKV // 2)
    def _(b):
        kfloat[...] = kraw[pl.ds(pl.multiple_of(2 * CACHE + b * 512, 512), 512), :].astype(F32)
        for c in range(2):
            flat = kfloat[pl.ds(c, 256, 2), :].astype(BF16)
            for s in range(2):
                kd[2 * b + s, :, c * DH : (c + 1) * DH] = flat[s * SEQC : (s + 1) * SEQC]

    def z_wait_y_send(j):
        z_all(j).wait_recv()
        y_copy(j, 0).start()
        y_copy(j, 1).start()

    def y_copy(j, side):
        tile = qtile(j, y)
        return rcopy(tile, tile, ys.at[j, side], yr.at[j, side], z * NY + (yp if side == 0 else ym))

    def half_of(view, j, side):
        h = NZ * rows_of(j) // 2
        return view.at[pl.ds(side * h, h), :]

    def h_copy(j, side):
        part = half_of(qtile(j, ym if side == 0 else yp), j, side)
        return rcopy(part, part, hs.at[j, side], hr.at[j, side], z * NY + (yp if side == 0 else ym))

    def y_wait_fwd(j):
        for side in (0, 1):
            tile = qtile(j, ym if side == 0 else yp)
            rcopy(tile, tile, ys.at[j, side], yr.at[j, side], z * NY + yp).wait_recv()
            h_copy(j, side).start()

    def h_wait(j):
        for side in (0, 1):
            part = half_of(qtile(j, y2), j, side)
            rcopy(part, part, hs.at[j, side], hr.at[j, side], z * NY + yp).wait_recv()

    def s_copy(j, yt):
        return rcopy(
            stat.at[j * NY + yt], srecv.at[j, me], ss.at[j, yt], sr.at[j], STAT_Z[j] * NY + yt
        )

    def stats_send(j):
        for yt in range(NY):
            target = STAT_Z[j] * NY + yt

            @pl.when(target != me)
            def _():
                s_copy(j, yt).start()

            @pl.when(target == me)
            def _():
                srecv[j, me] = stat[j * NY + yt]

    def r_copy(j, target):
        return rcopy(ressend.at[j], res.at[j * NY + y], rs.at[j], rr.at[j, y], target)

    def stats_own(j):
        @pl.when(z == STAT_Z[j])
        def _():
            most = srecv.at[j, pl.ds(0, NKV - 1)]
            rcopy(most, most, rs.at[j], sr.at[j], z * NY + yp).wait_recv()
            every = srecv[j]
            best = jnp.max(every[:, 0:4, :], axis=0)
            norm = jnp.sum(every[:, 4:8, :] * jnp.exp2((every[:, 0:4, :] - best[None]) * EXPC), axis=0)
            both = jnp.concatenate([best, 1.0 / norm], axis=0)
            ressend[j] = both
            res[j * NY + y] = both

            @pl.loop(1, NKV)
            def _(d):
                r_copy(j, (me + d) % NKV).start()

    def stats_wait(j):
        for yt in range(NY):
            owner = STAT_Z[j] * NY + yt

            @pl.when(owner != me)
            def _():
                rcopy(ressend.at[j], res.at[j * NY + yt], rs.at[j], rr.at[j, yt], owner).wait_recv()

    def combine(j):
        @pl.loop(0, NY)
        def _(yy):
            tt = j * NY + yy
            factors = []
            for c in range(2):
                pick = lambda ref, lo: jnp.concatenate(
                    [ref[tt, lo + 2 * c + hh : lo + 2 * c + hh + 1, :] for hh in range(2)], axis=1
                )
                factors.append(jnp.exp2((pick(stat, 0) - pick(res, 0)) * EXPC) * pick(res, 4))
            both = oacc[tt, 0] * factors[0] - oacc[tt, 1] * (factors[1] * mix[0])
            comb[tt] = both.T.astype(BF16)

    def x_copy(j, side):
        part = half_of(ctile(j, y2), j, side)
        return rcopy(part, rh.at[j, side], xs.at[j, side], xr.at[j, side], z * NY + (yp if side == 0 else ym))

    def f_copy(j, side):
        tile = ctile(j, yp if side == 0 else ym)
        return rcopy(tile, rf.at[j, side], fs.at[j, side], fr.at[j, side], z * NY + (yp if side == 0 else ym))

    def rs_first(j):
        stats_wait(j)
        combine(j)
        for side in (0, 1):
            x_copy(j, side).start()

    def rs_second(j):
        for side in (0, 1):
            x_copy(j, side).wait_recv()
            part = half_of(ctile(j, yp if side == 0 else ym), j, side)
            part[...] = (part[...].astype(F32) + rh[j, side].astype(F32)).astype(BF16)
            f_copy(j, side).start()

    def w_copy(j, d):
        zt = (z + d) % NZ
        return rcopy(zblock(accb.at[j], zt, R), rz.at[j, d - 1], ws.at[j], wr.at[j], zt * NY + y)

    def w_all(j):
        return rcopy(rz.at[j], rz.at[j], ws.at[j], wr.at[j], z * NY + yp)

    def rs_third(j):
        for side in (0, 1):
            f_copy(j, side).wait_recv()
        total = comb[j * NY + y].astype(F32) + rf[j, 0].astype(F32) + rf[j, 1].astype(F32)
        accb[j] = total.astype(BF16)
        acc[j] = total
        for d in (4, 3, 5, 2, 6, 1, 7):
            w_copy(j, d).start()

    def rs_last(j):
        total = acc[j, pl.ds(pl.multiple_of(z * R, R), R), :]
        w_all(j).wait_recv()
        for d in range(NZ - 1):
            total = total + rz[j, d].astype(F32)
        mixed[j * R : (j + 1) * R, :] = total

    def span(j):
        return slice(j * R, j * R + rows_of(j))

    def p_copy(j):
        return tcopy(
            term.at[1 - core, :, span(j), :], pr.at[:, span(j), :], ps.at[j], ps_r.at[j], x, 1 - core
        )

    def project_out(j):
        n = rows_of(j)
        total = mixed[span(j), :]
        inv_rms = lax.rsqrt(jnp.mean(total * total, axis=-1, keepdims=True) + EPS)
        head = (total * inv_rms * gain_ref[...] * OUT_SCALE).astype(BF16)
        for tx in range(NX):
            for tc in range(2):
                at = (tx * 2 + tc) * OUTB
                one = jnp.dot(head, wo[:, at : at + OUTB], preferred_element_type=F32)
                term[tc, tx, span(j), :] = one.astype(BF16)
        p_copy(j).start()

    def t_copy(j, side):
        cols = slice(side * OUTB // 2, (side + 1) * OUTB // 2)
        return tcopy(
            tsum.at[x2, span(j), cols], th.at[side, span(j), :], ts.at[j, side], tr.at[j, side],
            xp if side == 0 else xm, core,
        )

    def u_copy(j, side):
        to = xp if side == 0 else xm
        return tcopy(tsum.at[to, span(j), :], tf.at[side, span(j), :], us.at[j, side], ur.at[j, side], to, core)

    def tp_first(j):
        p_copy(j).wait_recv()
        for tx in range(NX):
            both = term[core, tx, span(j), :].astype(F32) + pr[tx, span(j), :].astype(F32)
            tsum[tx, span(j), :] = both.astype(BF16)
        for side in (0, 1):
            t_copy(j, side).start()

    def tp_second(j):
        for side in (0, 1):
            t_copy(j, side).wait_recv()
            to = xp if side == 0 else xm
            cols = slice(side * OUTB // 2, (side + 1) * OUTB // 2)
            both = tsum[to, span(j), cols].astype(F32) + th[side, span(j), :].astype(F32)
            tsum[to, span(j), cols] = both.astype(BF16)
            u_copy(j, side).start()

    def tp_last(j):
        for side in (0, 1):
            u_copy(j, side).wait_recv()
        own = term[core, x, span(j), :].astype(F32) + pr[x, span(j), :].astype(F32)
        total = (own + tf[0, span(j), :].astype(F32) + tf[1, span(j), :].astype(F32)).astype(BF16)
        if j < CHUNKS:
            piece_ref[span(j), :] = total
        else:
            step_ref[...] = total[:1]

    KB = [(b * 256, 256) for b in range(CACHE // 256)] + [(CACHE, 128)]

    @pl.loop(0, CHUNKS * NY)
    def _(t):
        for step, work, arg in (
            (0, z_wait_y_send, 0),
            (1, z_wait_y_send, 1),
            (1, y_wait_fwd, 0),
            (2, z_wait_y_send, 2),
            (3, h_wait, 0),
            (3, z_wait_y_send, 3),
            (4, stats_send, 0),
            (4, y_wait_fwd, 1),
            (5, y_wait_fwd, 2),
            (6, y_wait_fwd, 3),
            (7, h_wait, 1),
            (7, stats_own, 0),
            (8, stats_send, 1),
            (10, rs_first, 0),
            (11, h_wait, 2),
            (11, stats_own, 1),
            (11, rs_second, 0),
        ):
            pl.when(t == step)(functools.partial(work, arg))

        j = t // NY
        i = t % NY
        yy = (y + jnp.where(i == 2, 3, jnp.where(i == 3, 2, i))) % NY
        tt = j * NY + yy
        lane = lax.broadcasted_iota(jnp.int32, (128, TILE), 1)
        row = lax.broadcasted_iota(jnp.int32, (128, TILE), 0)
        row_place = ((lane // R) * NY + yy) * ROWS + R * j + lane % R
        fresh_ok = (row < ROWS) & (me * ROWS + row <= row_place)
        for c in range(2):
            cols = slice(c * DH, (c + 1) * DH)
            q = qall[tt, :, cols]
            top = jnp.full((8, TILE), -jnp.inf, F32)
            for at, size in KB:
                s = lax.dot_general(kbuf[at : at + size, cols], q, NT, preferred_element_type=F32)
                if at == CACHE:
                    s = jnp.where(fresh_ok, s, -jnp.inf)
                elif at >= half:
                    b = bias[at - half : at - half + size, :]
                    s = s + jnp.concatenate([b, b], axis=1)
                sbuf[c, at : at + size, :] = s
                top = jnp.maximum(top, jnp.max(s.reshape(size // 8, 8, TILE), axis=0))
            m = jnp.max(top, axis=0, keepdims=True)
            total = jnp.zeros((8, TILE), F32)
            for at, size in KB:
                w = jnp.exp2((sbuf[c, at : at + size, :] - m) * EXPC)
                total = total + jnp.sum(w.reshape(size // 8, 8, TILE), axis=0)
                pbuf[c, at : at + size, :] = w.astype(BF16)
            total = jnp.sum(total, axis=0, keepdims=True)
            oacc[tt, c] = jnp.dot(vt[...], pbuf[c], preferred_element_type=F32)
            for hh in range(2):
                stat[tt, 2 * c + hh : 2 * c + hh + 1, :] = m[:, hh * 128 : (hh + 1) * 128]
                stat[tt, 4 + 2 * c + hh : 5 + 2 * c + hh, :] = total[:, hh * 128 : (hh + 1) * 128]

    stats_send(2)

    loads[4].wait()
    h_wait(3)

    @pl.loop(0, NY)
    def _(yy):
        q2 = qd[yy]
        lane = lax.broadcasted_iota(jnp.int32, (SEQC, TILED), 1)
        row = lax.broadcasted_iota(jnp.int32, (SEQC, TILED), 0)
        own = (lane // RD == jnp.where(yy == y, z, NZ)) & (row == 0)
        limit = jnp.zeros((SEQC, TILED), jnp.int32)
        for zz in range(NZ):
            vtd[:, zz * SEQC : (zz + 1) * SEQC] = vdn[zz * NY + yy].T
            limit = jnp.where(lane // RD == zz, slens[zz * NY + yy], limit)
        seen = me * SEQC + row < limit
        for c in range(2):
            cols = slice(c * DH, (c + 1) * DH)
            q = q2[:, cols]
            s = jnp.full((SEQC, TILED), -jnp.inf, F32)
            for zz in range(NZ):
                one = lax.dot_general(kd[zz * NY + yy, :, cols], q, NT, preferred_element_type=F32)
                s = jnp.where((lane // RD == zz) & seen, one, s)
            extra = lax.dot_general(ksd[:, cols], q, NT, preferred_element_type=F32)
            extra = jnp.where(own, extra, -jnp.inf)
            m = jnp.max(jnp.maximum(s, extra), axis=0, keepdims=True)
            w = jnp.exp2((s - m) * EXPC)
            we = jnp.exp2((extra - m) * EXPC)
            total = jnp.sum(w + we, axis=0, keepdims=True)
            out = jnp.dot(vse[...], we.astype(BF16), preferred_element_type=F32)
            for zz in range(NZ):
                part = jnp.where(lane // RD == zz, w, 0.0).astype(BF16)
                out = out + jnp.dot(
                    vtd[:, zz * SEQC : (zz + 1) * SEQC], part, preferred_element_type=F32
                )
            out = out.T
            for zz in range(NZ):
                b = zz * NY + yy
                for hh in range(2):
                    dsend[b, 2 * c + hh : 2 * c + hh + 1, :] = out[
                        RD * zz : RD * zz + 1, hh * 128 : (hh + 1) * 128
                    ]
                dsend[b, 4 + c : 5 + c, :] = m
                dsend[b, 6 + c : 7 + c, :] = total

    def d_copy(target):
        return rcopy(dsend.at[target], drecv.at[me], ds.at[0], dr.at[0], target)

    @pl.loop(1, NKV)
    def _(d):
        d_copy((me + d) % NKV).start()

    drecv[me] = dsend[me]

    def d_all():
        most = drecv.at[pl.ds(0, NKV - 1)]
        return rcopy(most, most, ds.at[0], dr.at[0], z * NY + yp)

    def decode_row():
        d_all().wait_recv()
        mine = lax.broadcasted_iota(jnp.int32, (NKV, 128), 1) == RD * z
        parts = []
        for c in range(2):
            pick = lambda at: jnp.sum(jnp.where(mine, drecv[:, at, :], 0.0), axis=1, keepdims=True)
            m = pick(4 + c)
            scale = jnp.exp2((m - jnp.max(m, axis=0, keepdims=True)) * EXPC)
            norm = jnp.sum(pick(6 + c) * scale, axis=0, keepdims=True)
            parts.append(
                [jnp.sum(drecv[:, 2 * c + hh, :] * scale, axis=0, keepdims=True) / norm for hh in range(2)]
            )
        for hh in range(2):
            mixed[ROWS : ROWS + 1, hh * 128 : (hh + 1) * 128] = parts[0][hh] - mix[0] * parts[1][hh]

    rs_third(0)
    rs_first(1)
    stats_own(2)
    rs_second(1)
    rs_last(0)
    loads[5].wait()
    project_out(0)
    rs_third(1)
    rs_first(2)
    tp_first(0)
    rs_last(1)
    project_out(1)
    rs_second(2)
    tp_second(0)
    decode_row()
    project_out(3)
    rs_third(2)
    tp_first(1)
    tp_last(0)
    tp_first(3)
    tp_second(1)
    tp_second(3)
    rs_last(2)
    project_out(2)
    tp_last(1)
    tp_last(3)
    tp_first(2)
    tp_second(2)
    tp_last(2)

    for j in range(4):
        z_all(j).wait_send()
        p_copy(j).wait_send()
        for side in (0, 1):
            y_copy(j, side).wait_send()
            h_copy(j, side).wait_send()
            t_copy(j, side).wait_send()
            u_copy(j, side).wait_send()
    for j in range(CHUNKS):
        w_all(j).wait_send()
        for side in (0, 1):
            x_copy(j, side).wait_send()
            f_copy(j, side).wait_send()
        for yt in range(NY):

            @pl.when(STAT_Z[j] * NY + yt != me)
            def _():
                s_copy(j, yt).wait_send()

        @pl.when(z == STAT_Z[j])
        def _():
            most = srecv.at[j, pl.ds(0, NKV - 1)]
            rcopy(most, most, rs.at[j], sr.at[j], z * NY + yp).wait_send()

    d_all().wait_send()


def attention(q, k, normed, wv, kp, vp, kd, vd, wo, gain, prompt_len, step_lens, mix):
    vmem = pl.BlockSpec(memory_space=pltpu.VMEM)
    anyw = pl.BlockSpec(memory_space=pl.ANY)
    smem = pl.BlockSpec(memory_space=pltpu.SMEM)
    dma = pltpu.SemaphoreType.DMA
    V = pltpu.VMEM
    nt = CHUNKS * NY
    return pl.pallas_call(
        attend,
        out_shape=(
            jax.ShapeDtypeStruct((ROWS, OUTB), BF16),
            jax.ShapeDtypeStruct((1, OUTB), BF16),
            jax.ShapeDtypeStruct((ROWS, DV), BF16),
            jax.ShapeDtypeStruct((1, DV), BF16),
        ),
        in_specs=[vmem, vmem, vmem] + [anyw] * 6 + [vmem, smem, smem, smem],
        out_specs=(vmem,) * 4,
        scratch_shapes=[
            V((D, DV), BF16),
            V((DV, D), BF16),
            V((2 * CACHE + 2 * NKV * SEQC, DH), BF16),
            V((512, DH), F32),
            V((KEYS, 2 * DH), BF16),
            V((CACHE, DV), BF16),
            V((DV, KEYS), BF16),
            V((NKV, SEQC, 2 * DH), BF16),
            V((NKV, SEQC, DV), BF16),
            V((DV, NZ * SEQC), BF16),
            V((SEQC, 2 * DH), BF16),
            V((DV, SEQC), BF16),
            V((nt, TILE, 2 * DH), BF16),
            V((NY, TILED, 2 * DH), BF16),
            V((CACHE // 2, 128), F32),
            V((2, KEYS, TILE), F32),
            V((2, KEYS, TILE), BF16),
            V((nt, 2, DV, TILE), F32),
            V((nt, 8, 128), F32),
            V((CHUNKS, NKV, 8, 128), F32),
            V((CHUNKS, 8, 128), F32),
            V((nt, 8, 128), F32),
            V((NKV, 8, 128), F32),
            V((NKV, 8, 128), F32),
            V((nt, TILE, DV), BF16),
            V((CHUNKS, 2, TILE // 2, DV), BF16),
            V((CHUNKS, 2, TILE, DV), BF16),
            V((CHUNKS, TILE, DV), F32),
            V((CHUNKS, TILE, DV), BF16),
            V((CHUNKS, NZ - 1, R, DV), BF16),
            V((PADDED, DV), F32),
            V((2, NX, PADDED, OUTB), BF16),
            V((NX, PADDED, OUTB), BF16),
            V((NX, PADDED, OUTB), BF16),
            V((2, PADDED, OUTB // 2), BF16),
            V((2, PADDED, OUTB), BF16),
            dma((6,)),
            dma((4,)), dma((4,)),
            dma((4, 2)), dma((4, 2)),
            dma((4, 2)), dma((4, 2)),
            dma((3, NY)), dma((3,)),
            dma((3,)), dma((3, NY)),
            dma((3, 2)), dma((3, 2)),
            dma((3, 2)), dma((3, 2)),
            dma((3,)), dma((3,)),
            dma((1,)), dma((1,)),
            dma((4,)), dma((4,)),
            dma((4, 2)), dma((4, 2)),
            dma((4, 2)), dma((4, 2)),
        ],
        compiler_params=pltpu.CompilerParams(
            collective_id=0, has_side_effects=True, vmem_limit_bytes=62 << 20
        ),
        name="attend",
    )(q, k, normed, wv, kp, vp, kd, vd, wo, gain, prompt_len, step_lens, mix)


def norm_rows(tokens, in_gain):
    floats = tokens.astype(F32)
    inv_rms = lax.rsqrt(jnp.mean(floats * floats, axis=-1, keepdims=True) + EPS)
    return (floats * inv_rms * in_gain).astype(BF16)


def project(normed, weight):
    flat_weight = weight.reshape(weight.shape[0], -1)
    return jnp.dot(normed, flat_weight, preferred_element_type=F32).astype(BF16)


def on_device(
    piece_tokens, step_tokens, in_gain, w_query, w_key, w_value, w_out, mix_ratio, out_gain,
    prompt_keys, prompt_values, step_cache_keys, step_cache_values, prompt_len, step_lens,
):
    pad = jnp.zeros((RD - 1, piece_tokens.shape[1]), BF16)
    normed = norm_rows(jnp.concatenate([piece_tokens, step_tokens, pad], axis=0), in_gain)
    q = project(normed, w_query)
    k = project(normed, w_key)
    piece_out, step_out, piece_v, step_v = attention(
        q, k, normed, w_value.reshape(D, DV),
        prompt_keys.reshape(2 * CACHE, DH), prompt_values.reshape(CACHE, DV),
        step_cache_keys.reshape(2 * NKV * SEQC, DH), step_cache_values.reshape(NKV, SEQC, DV),
        w_out.reshape(DV, D), out_gain.reshape(1, DV), prompt_len, step_lens, mix_ratio,
    )
    return (
        piece_out, step_out,
        k[:ROWS].reshape(ROWS, 1, 2, DH), piece_v.reshape(ROWS, 1, DV),
        k[ROWS : ROWS + 1].reshape(1, 1, 2, DH), step_v.reshape(1, 1, DV),
    )


def solution(mesh):
    in_specs = (
        P("kv", None),
        P("kv", None),
        P(),
        P(None, "tp", None, None),
        P(None, "tp", None, None),
        P(None, "tp", None),
        P("tp", None, None),
        P("tp"),
        P(),
        P("kv", "tp", None, None),
        P("kv", "tp", None),
        P(None, "kv", "tp", None, None),
        P(None, "kv", "tp", None),
        P(),
        P(),
    )
    out_specs = (
        P("kv", "tp"),
        P("kv", "tp"),
        P("kv", "tp", None, None),
        P("kv", "tp", None),
        P("kv", "tp", None, None),
        P("kv", "tp", None),
    )
    return jax.shard_map(
        on_device, mesh=mesh, in_specs=in_specs, out_specs=out_specs, check_vma=False
    )
```

```python
import functools
import math

import jax
import jax.numpy as jnp
from jax import lax
from jax.experimental import pallas as pl
from jax.experimental.pallas import tpu as pltpu
from jax.sharding import PartitionSpec as P

EPS = 1e-06
OUT_SCALE = 0.8
NZ, NY, NKV, NX = 8, 4, 32, 4
D, OUTB = 4096, 512
ROWS = 96
CHUNKS = 3
R = ROWS // CHUNKS
RD = 16
TILE = NZ * R
COUNT = CHUNKS * NY
TILED = NZ * RD
CACHE = 2048
KEYS = CACHE + 128
SEQC = 128
DH, DV = 128, 256
PADDED = ROWS + RD
EXPC = DH ** (-0.5) * math.log2(math.e)
STAT_Z = (1, 4, 7)
F32, BF16 = jnp.float32, jnp.bfloat16
NT = (((1,), (1,)), ((), ()))


def attend(
    tok_hbm, step_tok, in_gain, wq_hbm, wk_hbm, wv_hbm, kp_hbm, vp_hbm, kd_hbm, vd_hbm, wo_hbm,
    gain_ref, plen, slens, mix,
    out_ref,
    tok, normed, wq, wk, wdeint, wv, wo, kraw, kfloat, kbuf, vnat, vt, kd, vdn, vtd, ksd, vse, qall, qd,
    bias, sbuf, pbuf, mrow, oacc,
    stat, srecv, ressend, res, dsend, drecv, comb, rh, rf, acc, accb, rz, mixed,
    term, tsum, pr, th, tf,
    load_sem, zs, zr, ys, yr, hs, hr, ss, sr, rs, rr, xs, xr, fs, fr, ws, wr, ds, dr,
    ps, ps_r, ts, tr, us, ur,
):
    me = lax.axis_index("kv")
    tp = lax.axis_index("tp")
    z = me // NY
    y = me % NY
    yp, ym, y2 = (y + 1) % NY, (y + 3) % NY, (y + 2) % NY
    x = tp // 2
    core = tp % 2
    xp, xm, x2 = (x + 1) % NX, (x + 3) % NX, (x + 2) % NX

    def at_kv(index):
        return {"kv": index}

    def rcopy(src, dst, s_sem, r_sem, target):
        return pltpu.make_async_remote_copy(
            src_ref=src, dst_ref=dst, send_sem=s_sem, recv_sem=r_sem,
            device_id=at_kv(target), device_id_type=pl.DeviceIdType.MESH,
        )

    def tcopy(src, dst, s_sem, r_sem, tx, tc):
        return pltpu.make_async_remote_copy(
            src_ref=src, dst_ref=dst, send_sem=s_sem, recv_sem=r_sem,
            device_id={"tp": tx * 2 + tc}, device_id_type=pl.DeviceIdType.MESH,
        )

    def rows_of(j):
        return R if j < CHUNKS else RD

    def qtile(j, yy):
        return qall.at[j * NY + yy] if j < CHUNKS else qd.at[yy]

    def ctile(j, yy):
        return comb.at[j * NY + yy]

    def zblock(view, zz, n):
        return view.at[pl.ds(pl.multiple_of(zz * n, n), n), :]

    barrier = pltpu.get_barrier_semaphore()

    @pl.loop(1, NKV)
    def _(d):
        pl.semaphore_signal(
            barrier, inc=1, device_id=at_kv((me + d) % NKV),
            device_id_type=pl.DeviceIdType.MESH,
        )

    for tx, tc in ((x, 1 - core), (xp, core), (xm, core)):
        pl.semaphore_signal(
            barrier, inc=1, device_id={"tp": tx * 2 + tc}, device_id_type=pl.DeviceIdType.MESH
        )

    loads = [
        pltpu.make_async_copy(tok_hbm, tok, load_sem.at[0]),
        pltpu.make_async_copy(wq_hbm, wq, load_sem.at[1]),
        pltpu.make_async_copy(wk_hbm, wk, load_sem.at[2]),
        pltpu.make_async_copy(wv_hbm, wv, load_sem.at[3]),
        pltpu.make_async_copy(kp_hbm, kraw.at[pl.ds(0, 2 * CACHE), :], load_sem.at[4]),
        pltpu.make_async_copy(vp_hbm, vnat, load_sem.at[5]),
        pltpu.make_async_copy(kd_hbm, kraw.at[pl.ds(2 * CACHE, 2 * NKV * SEQC), :], load_sem.at[6]),
        pltpu.make_async_copy(vd_hbm, vdn, load_sem.at[7]),
        pltpu.make_async_copy(wo_hbm, wo, load_sem.at[8]),
    ]
    for load in loads:
        load.start()

    def norm(rows):
        floats = rows.astype(F32)
        inv_rms = lax.rsqrt(jnp.mean(floats * floats, axis=-1, keepdims=True) + EPS)
        return (floats * inv_rms * in_gain[...]).astype(BF16)

    last = norm(step_tok[...])
    normed[ROWS:, :] = jnp.concatenate([last, jnp.zeros((RD - 1, D), BF16)], axis=0)
    loads[0].wait()

    @pl.loop(0, ROWS // 16)
    def _(b):
        rows = pl.ds(pl.multiple_of(b * 16, 16), 16)
        normed[rows, :] = norm(tok[rows, :])

    def split_maps(src, src_block, put):
        kfloat[...] = src[pl.ds(pl.multiple_of(src_block * 512, 512), 512), :].astype(F32)
        for c in range(2):
            put(c, kfloat[pl.ds(c, 256, 2), :].astype(BF16))

    def projected(weights):
        @pl.loop(0, D // 256)
        def _(b):
            def put(c, flat):
                rows = pl.ds(pl.multiple_of(b * 256, 256), 256)
                wdeint[rows, c * DH : (c + 1) * DH] = flat

            split_maps(weights, b, put)

        return jnp.dot(normed[...], wdeint[...], preferred_element_type=F32).astype(BF16)

    loads[1].wait()
    queries = projected(wq)
    for j in range(4):
        n = rows_of(j)
        lo = j * R if j < CHUNKS else ROWS
        mine = qtile(j, y)
        mine[pl.ds(pl.multiple_of(z * n, n), n), :] = queries[lo : lo + n, :]
    loads[2].wait()
    keys = projected(wk)
    out_ref[:, OUTB + DV :] = keys
    loads[3].wait()
    values = jnp.dot(normed[...], wv[...], preferred_element_type=F32).astype(BF16)
    out_ref[:, OUTB : OUTB + DV] = values

    kbuf[CACHE : CACHE + ROWS, :] = keys[:ROWS, :]
    kbuf[CACHE + ROWS :, :] = jnp.zeros((KEYS - CACHE - ROWS, 2 * DH), BF16)
    ksd[:RD, :] = keys[ROWS:, :]
    ksd[RD:, :] = jnp.zeros((SEQC - RD, 2 * DH), BF16)
    tail = jnp.concatenate([values[:ROWS, :], jnp.zeros((128 - ROWS, DV), BF16)], axis=0)
    vt[:, CACHE:] = tail.T
    tail = jnp.concatenate([values[ROWS:, :], jnp.zeros((128 - RD, DV), BF16)], axis=0)
    vse[...] = tail.T
    half = CACHE // 2
    place = me * CACHE + half + lax.broadcasted_iota(jnp.int32, (half, 128), 0)
    bias[...] = jnp.where(place < plen[0], 0.0, -jnp.inf).astype(F32)
    mixed[...] = jnp.zeros((PADDED, DV), F32)
    loads[4].wait()
    loads[5].wait()

    @pl.loop(0, CACHE // 256)
    def _(b):
        def put(c, flat):
            kbuf[pl.ds(pl.multiple_of(b * 256, 256), 256), c * DH : (c + 1) * DH] = flat

        split_maps(kraw, b, put)

    for b in range(CACHE // 256):
        vt[:, b * 256 : (b + 1) * 256] = vnat[b * 256 : (b + 1) * 256, :].T
    pl.semaphore_wait(barrier, NKV - 1 + 3)

    def z_copy(j, d):
        n = rows_of(j)
        zt = (z + d) % NZ
        block = zblock(qtile(j, y), z, n)
        return rcopy(block, block, zs.at[j], zr.at[j], zt * NY + y)

    def z_all(j):
        some = qtile(j, y).at[pl.ds(0, (NZ - 1) * rows_of(j)), :]
        return rcopy(some, some, zs.at[j], zr.at[j], z * NY + yp)

    for j in range(4):
        for d in (1, 7, 2, 6, 3, 5, 4):
            z_copy(j, d).start()

    loads[6].wait()

    @pl.loop(0, NKV // 2)
    def _(b):
        def put(c, flat):
            for part in range(2):
                kd[2 * b + part, :, c * DH : (c + 1) * DH] = flat[part * SEQC : (part + 1) * SEQC]

        split_maps(kraw, 2 * CACHE // 512 + b, put)

    def z_wait_y_send(j):
        z_all(j).wait_recv()
        y_copy(j, 0).start()
        y_copy(j, 1).start()

    def y_copy(j, side):
        tile = qtile(j, y)
        return rcopy(tile, tile, ys.at[j, side], yr.at[j, side], z * NY + (yp if side == 0 else ym))

    def half_of(view, j, side):
        h = NZ * rows_of(j) // 2
        return view.at[pl.ds(side * h, h), :]

    def h_copy(j, side):
        part = half_of(qtile(j, ym if side == 0 else yp), j, side)
        return rcopy(part, part, hs.at[j, side], hr.at[j, side], z * NY + (yp if side == 0 else ym))

    def y_wait_fwd(j):
        for side in (0, 1):
            tile = qtile(j, ym if side == 0 else yp)
            rcopy(tile, tile, ys.at[j, side], yr.at[j, side], z * NY + yp).wait_recv()
            h_copy(j, side).start()

    def h_wait(j):
        for side in (0, 1):
            part = half_of(qtile(j, y2), j, side)
            rcopy(part, part, hs.at[j, side], hr.at[j, side], z * NY + yp).wait_recv()

    def s_copy(j, yt):
        return rcopy(
            stat.at[j * NY + yt], srecv.at[j, me], ss.at[j, yt], sr.at[j], STAT_Z[j] * NY + yt
        )

    def stats_send(j):
        for yt in range(NY):
            target = STAT_Z[j] * NY + yt

            @pl.when(target != me)
            def _():
                s_copy(j, yt).start()

            @pl.when(target == me)
            def _():
                srecv[j, me] = stat[j * NY + yt]

    def r_copy(j, target):
        return rcopy(ressend.at[j], res.at[j * NY + y], rs.at[j], rr.at[j, y], target)

    def stats_own(j):
        @pl.when(z == STAT_Z[j])
        def _():
            most = srecv.at[j, pl.ds(0, NKV - 1)]
            rcopy(most, most, rs.at[j], sr.at[j], z * NY + yp).wait_recv()
            every = srecv[j]
            best = jnp.max(every[:, 0:4, :], axis=0)
            norm = jnp.sum(every[:, 4:8, :] * jnp.exp2((every[:, 0:4, :] - best[None]) * EXPC), axis=0)
            both = jnp.concatenate([best, 1.0 / norm], axis=0)
            ressend[j] = both
            res[j * NY + y] = both

            @pl.loop(1, NKV)
            def _(d):
                r_copy(j, (me + d) % NKV).start()

    def stats_wait(j):
        for yt in range(NY):
            owner = STAT_Z[j] * NY + yt

            @pl.when(owner != me)
            def _():
                rcopy(ressend.at[j], res.at[j * NY + yt], rs.at[j], rr.at[j, yt], owner).wait_recv()

    def combine(j):
        @pl.loop(0, NY)
        def _(yy):
            tt = j * NY + yy
            factors = []
            for c in range(2):
                pick = lambda ref, lo: jnp.concatenate(
                    [ref[tt, lo + 2 * c + hh : lo + 2 * c + hh + 1, :] for hh in range(2)], axis=1
                )
                factors.append(jnp.exp2((pick(stat, 0) - pick(res, 0)) * EXPC) * pick(res, 4))
            both = oacc[tt, 0] * factors[0] - oacc[tt, 1] * (factors[1] * mix[0])
            comb[tt] = both.T.astype(BF16)

    def x_copy(j, side):
        part = half_of(ctile(j, y2), j, side)
        return rcopy(part, rh.at[j, side], xs.at[j, side], xr.at[j, side], z * NY + (yp if side == 0 else ym))

    def f_copy(j, side):
        tile = ctile(j, yp if side == 0 else ym)
        return rcopy(tile, rf.at[j, side], fs.at[j, side], fr.at[j, side], z * NY + (yp if side == 0 else ym))

    def rs_first(j):
        stats_wait(j)
        combine(j)
        for side in (0, 1):
            x_copy(j, side).start()

    def rs_second(j):
        for side in (0, 1):
            x_copy(j, side).wait_recv()
            part = half_of(ctile(j, yp if side == 0 else ym), j, side)
            part[...] = (part[...].astype(F32) + rh[j, side].astype(F32)).astype(BF16)
            f_copy(j, side).start()

    def w_copy(j, d):
        zt = (z + d) % NZ
        return rcopy(zblock(accb.at[j], zt, R), rz.at[j, d - 1], ws.at[j], wr.at[j], zt * NY + y)

    def w_all(j):
        return rcopy(rz.at[j], rz.at[j], ws.at[j], wr.at[j], z * NY + yp)

    def rs_third(j):
        for side in (0, 1):
            f_copy(j, side).wait_recv()
        total = comb[j * NY + y].astype(F32) + rf[j, 0].astype(F32) + rf[j, 1].astype(F32)
        accb[j] = total.astype(BF16)
        acc[j] = total
        for d in (4, 3, 5, 2, 6, 1, 7):
            w_copy(j, d).start()

    def rs_last(j):
        total = acc[j, pl.ds(pl.multiple_of(z * R, R), R), :]
        w_all(j).wait_recv()
        for d in range(NZ - 1):
            total = total + rz[j, d].astype(F32)
        mixed[j * R : (j + 1) * R, :] = total

    def span(j):
        return slice(j * R, j * R + rows_of(j))

    def p_copy(j):
        return tcopy(
            term.at[1 - core, :, span(j), :], pr.at[:, span(j), :], ps.at[j], ps_r.at[j], x, 1 - core
        )

    def project_out(j):
        n = rows_of(j)
        total = mixed[span(j), :]
        inv_rms = lax.rsqrt(jnp.mean(total * total, axis=-1, keepdims=True) + EPS)
        head = (total * inv_rms * gain_ref[...] * OUT_SCALE).astype(BF16)
        for tx in range(NX):
            for tc in range(2):
                at = (tx * 2 + tc) * OUTB
                one = jnp.dot(head, wo[:, at : at + OUTB], preferred_element_type=F32)
                term[tc, tx, span(j), :] = one.astype(BF16)
        p_copy(j).start()

    def t_copy(j, side):
        cols = slice(side * OUTB // 2, (side + 1) * OUTB // 2)
        return tcopy(
            tsum.at[x2, span(j), cols], th.at[side, span(j), :], ts.at[j, side], tr.at[j, side],
            xp if side == 0 else xm, core,
        )

    def u_copy(j, side):
        to = xp if side == 0 else xm
        return tcopy(tsum.at[to, span(j), :], tf.at[side, span(j), :], us.at[j, side], ur.at[j, side], to, core)

    def tp_first(j):
        p_copy(j).wait_recv()
        for tx in range(NX):
            both = term[core, tx, span(j), :].astype(F32) + pr[tx, span(j), :].astype(F32)
            tsum[tx, span(j), :] = both.astype(BF16)
        for side in (0, 1):
            t_copy(j, side).start()

    def tp_second(j):
        for side in (0, 1):
            t_copy(j, side).wait_recv()
            to = xp if side == 0 else xm
            cols = slice(side * OUTB // 2, (side + 1) * OUTB // 2)
            both = tsum[to, span(j), cols].astype(F32) + th[side, span(j), :].astype(F32)
            tsum[to, span(j), cols] = both.astype(BF16)
            u_copy(j, side).start()

    def tp_last(j):
        for side in (0, 1):
            u_copy(j, side).wait_recv()
        own = term[core, x, span(j), :].astype(F32) + pr[x, span(j), :].astype(F32)
        total = (own + tf[0, span(j), :].astype(F32) + tf[1, span(j), :].astype(F32)).astype(BF16)
        out_ref[span(j), :OUTB] = total

    KB = [(b * 256, 256) for b in range(CACHE // 256)] + [(CACHE, 128)]

    def tile_of(t):
        i = t % NY
        yy = (y + jnp.where(i == 2, 3, jnp.where(i == 3, 2, i))) % NY
        return t // NY, yy, (t // NY) * NY + yy

    def piece_step(t):
        j, yy, ta = tile_of(jnp.minimum(t, COUNT - 1))
        tb = jnp.where((t >= 1) & (t <= COUNT), tile_of(jnp.maximum(t - 1, 0))[2], COUNT)
        tc = jnp.where(t >= 2, tile_of(jnp.maximum(t - 2, 0))[2], COUNT)
        lane = lax.broadcasted_iota(jnp.int32, (128, TILE), 1)
        row = lax.broadcasted_iota(jnp.int32, (128, TILE), 0)
        row_place = ((lane // R) * NY + yy) * ROWS + R * j + lane % R
        fresh_ok = (row < ROWS) & (me * ROWS + row <= row_place)
        for c in range(2):
            cols = slice(c * DH, (c + 1) * DH)
            q = qall[ta, :, cols]
            m = mrow[c, 0:1, :]
            top = jnp.full((8, TILE), -jnp.inf, F32)
            total = jnp.zeros((8, TILE), F32)
            out = jnp.zeros((DV, TILE), F32)
            for at, size in KB:
                out = out + jnp.dot(
                    vt[:, at : at + size], pbuf[c, at : at + size, :], preferred_element_type=F32
                )
                w = jnp.exp2((sbuf[c, at : at + size, :] - m) * EXPC)
                total = total + jnp.sum(w.reshape(size // 8, 8, TILE), axis=0)
                pbuf[c, at : at + size, :] = w.astype(BF16)
                s = lax.dot_general(kbuf[at : at + size, cols], q, NT, preferred_element_type=F32)
                if at == CACHE:
                    s = jnp.where(fresh_ok, s, -jnp.inf)
                elif at >= half:
                    b = bias[at - half : at - half + size, :]
                    s = s + jnp.concatenate([b, b], axis=1)
                sbuf[c, at : at + size, :] = s
                top = jnp.maximum(top, jnp.max(s.reshape(size // 8, 8, TILE), axis=0))
            oacc[tc, c] = out
            total = jnp.sum(total, axis=0, keepdims=True)
            for hh in range(2):
                stat[tb, 2 * c + hh : 2 * c + hh + 1, :] = m[:, hh * 128 : (hh + 1) * 128]
                stat[tb, 4 + 2 * c + hh : 5 + 2 * c + hh, :] = total[:, hh * 128 : (hh + 1) * 128]
            mrow[c, 0:1, :] = jnp.max(top, axis=0, keepdims=True)

    def decode_step(t):
        lane = lax.broadcasted_iota(jnp.int32, (SEQC, TILED), 1)
        row = lax.broadcasted_iota(jnp.int32, (SEQC, TILED), 0)
        jobs = []
        for part in range(2):
            yy = 2 * (t - COUNT - 2) + part
            q2 = qd[yy]
            own = (lane // RD == jnp.where(yy == y, z, NZ)) & (row == 0)
            limit = jnp.zeros((SEQC, TILED), jnp.int32)
            for zz in range(NZ):
                vtd[part, :, zz * SEQC : (zz + 1) * SEQC] = vdn[zz * NY + yy].T
                limit = jnp.where(lane // RD == zz, slens[zz * NY + yy], limit)
            seen = me * SEQC + row < limit
            for c in range(2):
                cols = slice(c * DH, (c + 1) * DH)
                q = q2[:, cols]
                s = jnp.full((SEQC, TILED), -jnp.inf, F32)
                for zz in range(NZ):
                    one = lax.dot_general(kd[zz * NY + yy, :, cols], q, NT, preferred_element_type=F32)
                    s = jnp.where((lane // RD == zz) & seen, one, s)
                extra = lax.dot_general(ksd[:, cols], q, NT, preferred_element_type=F32)
                jobs.append((part, yy, c, s, jnp.where(own, extra, -jnp.inf)))
        ready = []
        for part, yy, c, s, extra in jobs:
            m = jnp.max(jnp.maximum(s, extra), axis=0, keepdims=True)
            w = jnp.exp2((s - m) * EXPC)
            we = jnp.exp2((extra - m) * EXPC)
            total = jnp.sum(w + we, axis=0, keepdims=True)
            for zz in range(NZ):
                b = zz * NY + yy
                dsend[b, 4 + c : 5 + c, :] = m
                dsend[b, 6 + c : 7 + c, :] = total
            ready.append((part, yy, c, w, we))
        for part, yy, c, w, we in ready:
            out = jnp.dot(vse[...], we.astype(BF16), preferred_element_type=F32)
            for zz in range(NZ):
                some = jnp.where(lane // RD == zz, w, 0.0).astype(BF16)
                out = out + jnp.dot(
                    vtd[part, :, zz * SEQC : (zz + 1) * SEQC], some, preferred_element_type=F32
                )
            out = out.T
            for zz in range(NZ):
                for hh in range(2):
                    dsend[zz * NY + yy, 2 * c + hh : 2 * c + hh + 1, :] = out[
                        RD * zz : RD * zz + 1, hh * 128 : (hh + 1) * 128
                    ]

    loads[7].wait()
    loads[8].wait()

    @pl.loop(0, COUNT + 4)
    def _(t):
        for step, work, arg in (
            (0, z_wait_y_send, 0),
            (1, z_wait_y_send, 1),
            (1, y_wait_fwd, 0),
            (2, z_wait_y_send, 2),
            (3, h_wait, 0),
            (3, z_wait_y_send, 3),
            (4, y_wait_fwd, 1),
            (5, stats_send, 0),
            (6, y_wait_fwd, 2),
            (7, h_wait, 1),
            (8, y_wait_fwd, 3),
            (9, stats_send, 1),
            (9, stats_own, 0),
            (11, h_wait, 2),
            (13, rs_first, 0),
            (13, stats_own, 1),
            (13, stats_send, 2),
            (14, h_wait, 3),
            (15, rs_second, 0),
            (15, rs_first, 1),
        ):
            pl.when(t == step)(functools.partial(work, arg))
        pl.when(t < COUNT + 2)(functools.partial(piece_step, t))
        pl.when(t >= COUNT + 2)(functools.partial(decode_step, t))

    def d_copy(target):
        return rcopy(dsend.at[target], drecv.at[me], ds.at[0], dr.at[0], target)

    @pl.loop(1, NKV)
    def _(d):
        d_copy((me + d) % NKV).start()

    drecv[me] = dsend[me]

    def d_all():
        most = drecv.at[pl.ds(0, NKV - 1)]
        return rcopy(most, most, ds.at[0], dr.at[0], z * NY + yp)

    def decode_row():
        d_all().wait_recv()
        mine = lax.broadcasted_iota(jnp.int32, (NKV, 128), 1) == RD * z
        parts = []
        for c in range(2):
            pick = lambda at: jnp.sum(jnp.where(mine, drecv[:, at, :], 0.0), axis=1, keepdims=True)
            m = pick(4 + c)
            scale = jnp.exp2((m - jnp.max(m, axis=0, keepdims=True)) * EXPC)
            norm = jnp.sum(pick(6 + c) * scale, axis=0, keepdims=True)
            parts.append(
                [jnp.sum(drecv[:, 2 * c + hh, :] * scale, axis=0, keepdims=True) / norm for hh in range(2)]
            )
        for hh in range(2):
            mixed[ROWS : ROWS + 1, hh * 128 : (hh + 1) * 128] = parts[0][hh] - mix[0] * parts[1][hh]

    stats_own(2)
    rs_third(0)
    rs_second(1)
    rs_first(2)
    rs_third(1)
    rs_last(0)
    project_out(0)
    rs_second(2)
    decode_row()
    project_out(3)
    tp_first(0)
    rs_third(2)
    rs_last(1)
    project_out(1)
    tp_first(3)
    tp_second(0)
    tp_first(1)
    tp_second(3)
    tp_last(0)
    rs_last(2)
    project_out(2)
    tp_second(1)
    tp_last(3)
    tp_first(2)
    tp_last(1)
    tp_second(2)
    tp_last(2)

    for j in range(4):
        z_all(j).wait_send()
        p_copy(j).wait_send()
        for side in (0, 1):
            y_copy(j, side).wait_send()
            h_copy(j, side).wait_send()
            t_copy(j, side).wait_send()
            u_copy(j, side).wait_send()
    for j in range(CHUNKS):
        w_all(j).wait_send()
        for side in (0, 1):
            x_copy(j, side).wait_send()
            f_copy(j, side).wait_send()
        for yt in range(NY):

            @pl.when(STAT_Z[j] * NY + yt != me)
            def _():
                s_copy(j, yt).wait_send()

        @pl.when(z == STAT_Z[j])
        def _():
            most = srecv.at[j, pl.ds(0, NKV - 1)]
            rcopy(most, most, rs.at[j], sr.at[j], z * NY + yp).wait_send()

    d_all().wait_send()


def attention(tok, step_tok, in_gain, wq, wk, wv, kp, vp, kd, vd, wo, gain, prompt_len, step_lens, mix):
    vmem = pl.BlockSpec(memory_space=pltpu.VMEM)
    anyw = pl.BlockSpec(memory_space=pl.ANY)
    smem = pl.BlockSpec(memory_space=pltpu.SMEM)
    dma = pltpu.SemaphoreType.DMA
    V = pltpu.VMEM
    nt = CHUNKS * NY
    return pl.pallas_call(
        attend,
        out_shape=jax.ShapeDtypeStruct((PADDED, OUTB + 2 * DV), BF16),
        in_specs=[anyw, vmem, vmem] + [anyw] * 8 + [vmem, smem, smem, smem],
        out_specs=vmem,
        scratch_shapes=[
            V((ROWS, D), BF16),
            V((PADDED, D), BF16),
            V((2 * D, DH), BF16),
            V((2 * D, DH), BF16),
            V((D, 2 * DH), BF16),
            V((D, DV), BF16),
            V((DV, D), BF16),
            V((2 * CACHE + 2 * NKV * SEQC, DH), BF16),
            V((512, DH), F32),
            V((KEYS, 2 * DH), BF16),
            V((CACHE, DV), BF16),
            V((DV, KEYS), BF16),
            V((NKV, SEQC, 2 * DH), BF16),
            V((NKV, SEQC, DV), BF16),
            V((2, DV, NZ * SEQC), BF16),
            V((SEQC, 2 * DH), BF16),
            V((DV, SEQC), BF16),
            V((nt, TILE, 2 * DH), BF16),
            V((NY, TILED, 2 * DH), BF16),
            V((CACHE // 2, 128), F32),
            V((2, KEYS, TILE), F32),
            V((2, KEYS, TILE), BF16),
            V((2, 8, TILE), F32),
            V((nt + 1, 2, DV, TILE), F32),
            V((nt + 1, 8, 128), F32),
            V((CHUNKS, NKV, 8, 128), F32),
            V((CHUNKS, 8, 128), F32),
            V((nt, 8, 128), F32),
            V((NKV, 8, 128), F32),
            V((NKV, 8, 128), F32),
            V((nt, TILE, DV), BF16),
            V((CHUNKS, 2, TILE // 2, DV), BF16),
            V((CHUNKS, 2, TILE, DV), BF16),
            V((CHUNKS, TILE, DV), F32),
            V((CHUNKS, TILE, DV), BF16),
            V((CHUNKS, NZ - 1, R, DV), BF16),
            V((PADDED, DV), F32),
            V((2, NX, PADDED, OUTB), BF16),
            V((NX, PADDED, OUTB), BF16),
            V((NX, PADDED, OUTB), BF16),
            V((2, PADDED, OUTB // 2), BF16),
            V((2, PADDED, OUTB), BF16),
            dma((9,)),
            dma((4,)), dma((4,)),
            dma((4, 2)), dma((4, 2)),
            dma((4, 2)), dma((4, 2)),
            dma((3, NY)), dma((3,)),
            dma((3,)), dma((3, NY)),
            dma((3, 2)), dma((3, 2)),
            dma((3, 2)), dma((3, 2)),
            dma((3,)), dma((3,)),
            dma((1,)), dma((1,)),
            dma((4,)), dma((4,)),
            dma((4, 2)), dma((4, 2)),
            dma((4, 2)), dma((4, 2)),
        ],
        compiler_params=pltpu.CompilerParams(
            collective_id=0, has_side_effects=True, vmem_limit_bytes=62 << 20
        ),
        name="attend",
    )(tok, step_tok, in_gain, wq, wk, wv, kp, vp, kd, vd, wo, gain, prompt_len, step_lens, mix)


def split_outputs(all_ref, piece_ref, step_ref, pk_ref, pv_ref, sk_ref, sv_ref, flat):
    piece_ref[...] = all_ref[:ROWS, :OUTB]
    step_ref[...] = all_ref[ROWS : ROWS + 1, :OUTB]
    pv_ref[...] = all_ref[:ROWS, OUTB : OUTB + DV]
    sv_ref[...] = all_ref[ROWS : ROWS + 1, OUTB : OUTB + DV]
    for c in range(2):
        at = OUTB + DV + c * DH
        flat[pl.ds(c, PADDED, 2), :] = all_ref[:, at : at + DH].astype(F32)
    pk_ref[...] = flat[: 2 * ROWS, :].astype(BF16)
    sk_ref[...] = flat[2 * ROWS : 2 * ROWS + 2, :].astype(BF16)


def on_device(
    piece_tokens, step_tokens, in_gain, w_query, w_key, w_value, w_out, mix_ratio, out_gain,
    prompt_keys, prompt_values, step_cache_keys, step_cache_values, prompt_len, step_lens,
):
    together = attention(
        piece_tokens, step_tokens, in_gain.reshape(1, D),
        w_query.reshape(2 * D, DH), w_key.reshape(2 * D, DH), w_value.reshape(D, DV),
        prompt_keys.reshape(2 * CACHE, DH), prompt_values.reshape(CACHE, DV),
        step_cache_keys.reshape(2 * NKV * SEQC, DH), step_cache_values.reshape(NKV, SEQC, DV),
        w_out.reshape(DV, D), out_gain.reshape(1, DV), prompt_len, step_lens, mix_ratio,
    )
    shapes = ((ROWS, OUTB), (1, OUTB), (2 * ROWS, DH), (ROWS, DV), (2, DH), (1, DV))
    piece_out, step_out, piece_k, piece_v, step_k, step_v = pl.pallas_call(
        split_outputs,
        out_shape=tuple(jax.ShapeDtypeStruct(shape, BF16) for shape in shapes),
        scratch_shapes=[pltpu.VMEM((2 * PADDED, DH), F32)],
        name="split",
    )(together)
    return (
        piece_out, step_out,
        piece_k.reshape(ROWS, 1, 2, DH), piece_v.reshape(ROWS, 1, DV),
        step_k.reshape(1, 1, 2, DH), step_v.reshape(1, 1, DV),
    )


def solution(mesh):
    in_specs = (
        P("kv", None),
        P("kv", None),
        P(),
        P(None, "tp", None, None),
        P(None, "tp", None, None),
        P(None, "tp", None),
        P("tp", None, None),
        P("tp"),
        P(),
        P("kv", "tp", None, None),
        P("kv", "tp", None),
        P(None, "kv", "tp", None, None),
        P(None, "kv", "tp", None),
        P(),
        P(),
    )
    out_specs = (
        P("kv", "tp"),
        P("kv", "tp"),
        P("kv", "tp", None, None),
        P("kv", "tp", None),
        P("kv", "tp", None, None),
        P("kv", "tp", None),
    )
    return jax.shard_map(
        on_device, mesh=mesh, in_specs=in_specs, out_specs=out_specs, check_vma=False
    )
```

```python
import functools
import math

import jax
import jax.numpy as jnp
from jax import lax
from jax.experimental import pallas as pl
from jax.experimental.pallas import tpu as pltpu
from jax.sharding import PartitionSpec as P

EPS = 1e-06
OUT_SCALE = 0.8
NZ, NY, NKV, NX = 8, 4, 32, 4
D, OUTB = 4096, 512
ROWS = 96
CHUNKS = 3
R = ROWS // CHUNKS
RD = 16
TILE = NZ * R
COUNT = CHUNKS * NY
TILED = NZ * RD
CACHE = 2048
KEYS = CACHE + 128
SEQC = 128
DH, DV = 128, 256
PADDED = ROWS + RD
EXPC = DH ** (-0.5) * math.log2(math.e)
STAT_Z = (1, 4, 7)
BATCHES = ((0,), (1, 7), (2, 6), (3, 5, 4))
F32, BF16 = jnp.float32, jnp.bfloat16
NT = (((1,), (1,)), ((), ()))


def attend(
    tok_hbm, step_tok, in_gain, wq_hbm, wk_hbm, wv_hbm, kp_hbm, vp_hbm, kd_hbm, vd_hbm, wo_hbm,
    gain_ref, plen, slens, mix,
    out_ref,
    tok, normed, wq, wk, wdeint, wv, wo, kraw, kfloat, kbuf, vnat, vt, kd, vdn, vtd, ksd, vse, qall, qd,
    bias, sbuf, pbuf, mrow, oacc,
    stat, srecv, ressend, res, dsend, drecv, comb, rh, rf, acc, accb, rz, mixed,
    term, tsum, pr, tf,
    load_sem, zs, zr, ys, yr, hs, hr, ss, sr, rs, rr, xs, xr, fs, fr, ws, wr, ds, dr,
    ps, ps_r, us, ur,
):
    me = lax.axis_index("kv")
    tp = lax.axis_index("tp")
    z = me // NY
    y = me % NY
    yp, ym, y2 = (y + 1) % NY, (y + 3) % NY, (y + 2) % NY
    x = tp // 2
    core = tp % 2
    xp, xm, x2 = (x + 1) % NX, (x + 3) % NX, (x + 2) % NX

    def at_kv(index):
        return {"kv": index}

    def rcopy(src, dst, s_sem, r_sem, target):
        return pltpu.make_async_remote_copy(
            src_ref=src, dst_ref=dst, send_sem=s_sem, recv_sem=r_sem,
            device_id=at_kv(target), device_id_type=pl.DeviceIdType.MESH,
        )

    def tcopy(src, dst, s_sem, r_sem, tx, tc):
        return pltpu.make_async_remote_copy(
            src_ref=src, dst_ref=dst, send_sem=s_sem, recv_sem=r_sem,
            device_id={"tp": tx * 2 + tc}, device_id_type=pl.DeviceIdType.MESH,
        )

    def rows_of(j):
        return R if j < CHUNKS else RD

    def qtile(j, yy):
        return qall.at[j * NY + yy] if j < CHUNKS else qd.at[yy]

    def ctile(j, yy):
        return comb.at[j * NY + yy]

    def zblock(view, zz, n):
        return view.at[pl.ds(pl.multiple_of(zz * n, n), n), :]

    loads = [
        pltpu.make_async_copy(tok_hbm, tok, load_sem.at[0]),
        pltpu.make_async_copy(wq_hbm, wq, load_sem.at[1]),
        pltpu.make_async_copy(wk_hbm, wk, load_sem.at[2]),
        pltpu.make_async_copy(wv_hbm, wv, load_sem.at[3]),
        pltpu.make_async_copy(kp_hbm, kraw.at[pl.ds(0, 2 * CACHE), :], load_sem.at[4]),
        pltpu.make_async_copy(vp_hbm, vnat, load_sem.at[5]),
        pltpu.make_async_copy(kd_hbm, kraw.at[pl.ds(2 * CACHE, 2 * NKV * SEQC), :], load_sem.at[6]),
        pltpu.make_async_copy(vd_hbm, vdn, load_sem.at[7]),
        pltpu.make_async_copy(wo_hbm, wo, load_sem.at[8]),
    ]
    for load in loads[:2]:
        load.start()

    barrier = pltpu.get_barrier_semaphore()

    @pl.loop(1, NKV)
    def _(d):
        pl.semaphore_signal(
            barrier, inc=1, device_id=at_kv((me + d) % NKV),
            device_id_type=pl.DeviceIdType.MESH,
        )

    for tx, tc in ((x, 1 - core), (xp, core), (x2, core), (xm, core)):
        pl.semaphore_signal(
            barrier, inc=1, device_id={"tp": tx * 2 + tc}, device_id_type=pl.DeviceIdType.MESH
        )

    def norm(rows):
        floats = rows.astype(F32)
        inv_rms = lax.rsqrt(jnp.mean(floats * floats, axis=-1, keepdims=True) + EPS)
        return (floats * inv_rms * in_gain[...]).astype(BF16)

    last = norm(step_tok[...])
    normed[ROWS:, :] = jnp.concatenate([last, jnp.zeros((RD - 1, D), BF16)], axis=0)
    loads[0].wait()
    for load in loads[2:]:
        load.start()

    @pl.loop(0, ROWS // 16)
    def _(b):
        rows = pl.ds(pl.multiple_of(b * 16, 16), 16)
        normed[rows, :] = norm(tok[rows, :])

    def split_maps(src, src_block, put):
        kfloat[...] = src[pl.ds(pl.multiple_of(src_block * 512, 512), 512), :].astype(F32)
        for c in range(2):
            put(c, kfloat[pl.ds(c, 256, 2), :].astype(BF16))

    def projected(weights):
        @pl.loop(0, D // 256)
        def _(b):
            def put(c, flat):
                rows = pl.ds(pl.multiple_of(b * 256, 256), 256)
                wdeint[rows, c * DH : (c + 1) * DH] = flat

            split_maps(weights, b, put)

        return jnp.dot(normed[...], wdeint[...], preferred_element_type=F32).astype(BF16)

    loads[1].wait()
    queries = projected(wq)
    for j in range(4):
        n = rows_of(j)
        lo = j * R if j < CHUNKS else ROWS
        mine = qtile(j, y)
        mine[pl.ds(pl.multiple_of(z * n, n), n), :] = queries[lo : lo + n, :]

    def batch_sem(d):
        return {0: 0, 1: 1, 7: 1, 2: 2, 6: 2}.get(d, 3)

    def origin(d):
        return (z + NZ - d) % NZ

    def z_copy(j, d):
        block = zblock(qtile(j, y), z, rows_of(j))
        sem = zr.at[j, batch_sem(d)] if j < CHUNKS else zr.at[j, 0]
        return rcopy(block, block, zs.at[j], sem, ((z + d) % NZ) * NY + y)

    def z_some(j, count, sem):
        some = qtile(j, y).at[pl.ds(0, count * rows_of(j)), :]
        return rcopy(some, some, zs.at[j], sem, z * NY + yp)

    def z_all(j):
        return z_some(j, NZ - 1, zr.at[j, 0])

    def z_send(j):
        for d in (4, 3, 5, 2, 6, 1, 7):
            z_copy(j, d).start()

    def side_kv(side):
        return z * NY + (yp if side == 0 else ym)

    def z_relay(j, k):
        if k > 0:
            z_some(j, len(BATCHES[k]), zr.at[j, k]).wait_recv()
        for d in BATCHES[k]:
            block = zblock(qtile(j, y), origin(d), R)
            for side in (0, 1):
                rcopy(block, block, ys.at[j, side], yr.at[j, k], side_kv(side)).start()

    def y_relay(j, k):
        z_some(j, 2 * len(BATCHES[k]), yr.at[j, k]).wait_recv()
        for side in (0, 1):
            for d in BATCHES[k]:
                if (side == 0) == (d < NZ // 2):
                    block = zblock(qtile(j, ym if side == 0 else yp), origin(d), R)
                    rcopy(block, block, hs.at[j, side], hr.at[j, 0], side_kv(side)).start()

    pl.semaphore_wait(barrier, NKV - 1 + 4)
    z_send(0)
    z_relay(0, 0)

    loads[2].wait()
    keys = projected(wk)
    out_ref[:, OUTB + DV :] = keys
    loads[3].wait()
    values = jnp.dot(normed[...], wv[...], preferred_element_type=F32).astype(BF16)
    out_ref[:, OUTB : OUTB + DV] = values

    kbuf[CACHE : CACHE + ROWS, :] = keys[:ROWS, :]
    kbuf[CACHE + ROWS :, :] = jnp.zeros((KEYS - CACHE - ROWS, 2 * DH), BF16)
    ksd[:RD, :] = keys[ROWS:, :]
    ksd[RD:, :] = jnp.zeros((SEQC - RD, 2 * DH), BF16)
    tail = jnp.concatenate([values[:ROWS, :], jnp.zeros((128 - ROWS, DV), BF16)], axis=0)
    vt[:, CACHE:] = tail.T
    tail = jnp.concatenate([values[ROWS:, :], jnp.zeros((128 - RD, DV), BF16)], axis=0)
    vse[...] = tail.T
    half = CACHE // 2
    place = me * CACHE + half + lax.broadcasted_iota(jnp.int32, (half, 128), 0)
    bias[...] = jnp.where(place < plen[0], 0.0, -jnp.inf).astype(F32)
    mixed[...] = jnp.zeros((PADDED, DV), F32)
    loads[4].wait()
    loads[5].wait()

    @pl.loop(0, CACHE // 256)
    def _(b):
        def put(c, flat):
            kbuf[pl.ds(pl.multiple_of(b * 256, 256), 256), c * DH : (c + 1) * DH] = flat

        split_maps(kraw, b, put)

    for b in range(CACHE // 256):
        vt[:, b * 256 : (b + 1) * 256] = vnat[b * 256 : (b + 1) * 256, :].T
    loads[6].wait()

    @pl.loop(0, NKV // 2)
    def _(b):
        def put(c, flat):
            for part in range(2):
                kd[2 * b + part, :, c * DH : (c + 1) * DH] = flat[part * SEQC : (part + 1) * SEQC]

        split_maps(kraw, 2 * CACHE // 512 + b, put)

    def z_wait_y_send(j):
        z_all(j).wait_recv()
        y_copy(j, 0).start()
        y_copy(j, 1).start()

    def y_copy(j, side):
        tile = qtile(j, y)
        sem = yr.at[j, side]
        return rcopy(tile, tile, ys.at[j, side], sem, side_kv(side))

    def half_of(view, j, side):
        h = NZ * rows_of(j) // 2
        return view.at[pl.ds(side * h, h), :]

    def h_copy(j, side):
        part = half_of(qtile(j, ym if side == 0 else yp), j, side)
        return rcopy(part, part, hs.at[j, side], hr.at[j, side], side_kv(side))

    def y_wait_fwd(j):
        for side in (0, 1):
            tile = qtile(j, ym if side == 0 else yp)
            rcopy(tile, tile, ys.at[j, side], yr.at[j, side], z * NY + yp).wait_recv()
            h_copy(j, side).start()

    def h_wait(j):
        if j < CHUNKS:
            tile = qtile(j, y2)
            rcopy(tile, tile, hs.at[j, 0], hr.at[j, 0], z * NY + yp).wait_recv()
            return
        for side in (0, 1):
            part = half_of(qtile(j, y2), j, side)
            rcopy(part, part, hs.at[j, side], hr.at[j, side], z * NY + yp).wait_recv()

    def s_copy(j, yt):
        return rcopy(
            stat.at[j * NY + yt], srecv.at[j, me], ss.at[j, yt], sr.at[j], STAT_Z[j] * NY + yt
        )

    def stats_send(j):
        for yt in range(NY):
            target = STAT_Z[j] * NY + yt

            @pl.when(target != me)
            def _():
                s_copy(j, yt).start()

            @pl.when(target == me)
            def _():
                srecv[j, me] = stat[j * NY + yt]

    def r_copy(j, target):
        return rcopy(ressend.at[j], res.at[j * NY + y], rs.at[j], rr.at[j, y], target)

    def stats_own(j):
        @pl.when(z == STAT_Z[j])
        def _():
            most = srecv.at[j, pl.ds(0, NKV - 1)]
            rcopy(most, most, rs.at[j], sr.at[j], z * NY + yp).wait_recv()
            every = srecv[j]
            best = jnp.max(every[:, 0:4, :], axis=0)
            norm = jnp.sum(every[:, 4:8, :] * jnp.exp2((every[:, 0:4, :] - best[None]) * EXPC), axis=0)
            both = jnp.concatenate([best, 1.0 / norm], axis=0)
            ressend[j] = both
            res[j * NY + y] = both

            @pl.loop(1, NKV)
            def _(d):
                r_copy(j, (me + d) % NKV).start()

    def stats_wait(j):
        for yt in range(NY):
            owner = STAT_Z[j] * NY + yt

            @pl.when(owner != me)
            def _():
                rcopy(ressend.at[j], res.at[j * NY + yt], rs.at[j], rr.at[j, yt], owner).wait_recv()

    def combine(j):
        @pl.loop(0, NY)
        def _(yy):
            tt = j * NY + yy
            factors = []
            for c in range(2):
                pick = lambda ref, lo: jnp.concatenate(
                    [ref[tt, lo + 2 * c + hh : lo + 2 * c + hh + 1, :] for hh in range(2)], axis=1
                )
                factors.append(jnp.exp2((pick(stat, 0) - pick(res, 0)) * EXPC) * pick(res, 4))
            both = oacc[tt, 0] * factors[0] - oacc[tt, 1] * (factors[1] * mix[0])
            comb[tt] = both.T.astype(BF16)

    def x_copy(j, side):
        part = half_of(ctile(j, y2), j, side)
        return rcopy(part, rh.at[j, side], xs.at[j, side], xr.at[j, side], z * NY + (yp if side == 0 else ym))

    def f_copy(j, side):
        tile = ctile(j, yp if side == 0 else ym)
        return rcopy(tile, rf.at[j, side], fs.at[j, side], fr.at[j, side], z * NY + (yp if side == 0 else ym))

    def rs_first(j):
        stats_wait(j)
        combine(j)
        for side in (0, 1):
            x_copy(j, side).start()

    def rs_second(j):
        for side in (0, 1):
            x_copy(j, side).wait_recv()
            part = half_of(ctile(j, yp if side == 0 else ym), j, side)
            part[...] = (part[...].astype(F32) + rh[j, side].astype(F32)).astype(BF16)
            f_copy(j, side).start()

    def w_copy(j, d):
        zt = (z + d) % NZ
        return rcopy(zblock(accb.at[j], zt, R), rz.at[j, d - 1], ws.at[j], wr.at[j], zt * NY + y)

    def w_all(j):
        return rcopy(rz.at[j], rz.at[j], ws.at[j], wr.at[j], z * NY + yp)

    def rs_third(j):
        for side in (0, 1):
            f_copy(j, side).wait_recv()
        total = comb[j * NY + y].astype(F32) + rf[j, 0].astype(F32) + rf[j, 1].astype(F32)
        accb[j] = total.astype(BF16)
        acc[j] = total
        for d in (4, 3, 5, 2, 6, 1, 7):
            w_copy(j, d).start()

    def rs_last(j):
        total = acc[j, pl.ds(pl.multiple_of(z * R, R), R), :]
        w_all(j).wait_recv()
        for d in range(NZ - 1):
            total = total + rz[j, d].astype(F32)
        mixed[j * R : (j + 1) * R, :] = total

    def span(j):
        return slice(j * R, j * R + rows_of(j))

    def p_copy(j):
        return tcopy(
            term.at[1 - core, :, span(j), :], pr.at[:, span(j), :], ps.at[j], ps_r.at[j], x, 1 - core
        )

    def project_out(j):
        n = rows_of(j)
        total = mixed[span(j), :]
        inv_rms = lax.rsqrt(jnp.mean(total * total, axis=-1, keepdims=True) + EPS)
        head = (total * inv_rms * gain_ref[...] * OUT_SCALE).astype(BF16)
        for tx in range(NX):
            for tc in range(2):
                at = (tx * 2 + tc) * OUTB
                one = jnp.dot(head, wo[:, at : at + OUTB], preferred_element_type=F32)
                term[tc, tx, span(j), :] = one.astype(BF16)
        p_copy(j).start()

    def u_copy(j, d):
        to = (x + d) % NX
        return tcopy(tsum.at[to, span(j), :], tf.at[d - 1, span(j), :], us.at[j], ur.at[j], to, core)

    def u_all(j):
        some = tf.at[:, span(j), :]
        return tcopy(some, some, us.at[j], ur.at[j], xp, core)

    def tp_first(j):
        p_copy(j).wait_recv()
        for tx in range(NX):
            both = term[core, tx, span(j), :].astype(F32) + pr[tx, span(j), :].astype(F32)
            tsum[tx, span(j), :] = both.astype(BF16)
        for d in (2, 1, 3):
            u_copy(j, d).start()

    def tp_last(j):
        u_all(j).wait_recv()
        total = term[core, x, span(j), :].astype(F32) + pr[x, span(j), :].astype(F32)
        for d in range(NX - 1):
            total = total + tf[d, span(j), :].astype(F32)
        out_ref[span(j), :OUTB] = total.astype(BF16)

    KB = [(b * 256, 256) for b in range(CACHE // 256)] + [(CACHE, 128)]

    def tile_of(t):
        i = t % NY
        yy = (y + jnp.where(i == 2, 3, jnp.where(i == 3, 2, i))) % NY
        return t // NY, yy, (t // NY) * NY + yy

    def piece_step(t):
        j, yy, ta = tile_of(jnp.minimum(t, COUNT - 1))
        tb = jnp.where((t >= 1) & (t <= COUNT), tile_of(jnp.maximum(t - 1, 0))[2], COUNT)
        tc = jnp.where(t >= 2, tile_of(jnp.maximum(t - 2, 0))[2], COUNT)
        lane = lax.broadcasted_iota(jnp.int32, (128, TILE), 1)
        row = lax.broadcasted_iota(jnp.int32, (128, TILE), 0)
        row_place = ((lane // R) * NY + yy) * ROWS + R * j + lane % R
        fresh_ok = (row < ROWS) & (me * ROWS + row <= row_place)
        for c in range(2):
            cols = slice(c * DH, (c + 1) * DH)
            q = qall[ta, :, cols]
            m = mrow[c, 0:1, :]
            top = jnp.full((8, TILE), -jnp.inf, F32)
            total = jnp.zeros((8, TILE), F32)
            out = jnp.zeros((DV, TILE), F32)
            for at, size in KB:
                out = out + jnp.dot(
                    vt[:, at : at + size], pbuf[c, at : at + size, :], preferred_element_type=F32
                )
                w = jnp.exp2((sbuf[c, at : at + size, :] - m) * EXPC)
                total = total + jnp.sum(w.reshape(size // 8, 8, TILE), axis=0)
                pbuf[c, at : at + size, :] = w.astype(BF16)
                s = lax.dot_general(kbuf[at : at + size, cols], q, NT, preferred_element_type=F32)
                if at == CACHE:
                    s = jnp.where(fresh_ok, s, -jnp.inf)
                elif at >= half:
                    b = bias[at - half : at - half + size, :]
                    s = s + jnp.concatenate([b, b], axis=1)
                sbuf[c, at : at + size, :] = s
                top = jnp.maximum(top, jnp.max(s.reshape(size // 8, 8, TILE), axis=0))
            oacc[tc, c] = out
            total = jnp.sum(total, axis=0, keepdims=True)
            for hh in range(2):
                stat[tb, 2 * c + hh : 2 * c + hh + 1, :] = m[:, hh * 128 : (hh + 1) * 128]
                stat[tb, 4 + 2 * c + hh : 5 + 2 * c + hh, :] = total[:, hh * 128 : (hh + 1) * 128]
            mrow[c, 0:1, :] = jnp.max(top, axis=0, keepdims=True)

    def decode_step(t):
        lane = lax.broadcasted_iota(jnp.int32, (SEQC, TILED), 1)
        row = lax.broadcasted_iota(jnp.int32, (SEQC, TILED), 0)
        jobs = []
        for part in range(2):
            yy = 2 * (t - COUNT - 2) + part
            q2 = qd[yy]
            own = (lane // RD == jnp.where(yy == y, z, NZ)) & (row == 0)
            limit = jnp.zeros((SEQC, TILED), jnp.int32)
            for zz in range(NZ):
                vtd[part, :, zz * SEQC : (zz + 1) * SEQC] = vdn[zz * NY + yy].T
                limit = jnp.where(lane // RD == zz, slens[zz * NY + yy], limit)
            seen = me * SEQC + row < limit
            for c in range(2):
                cols = slice(c * DH, (c + 1) * DH)
                q = q2[:, cols]
                s = jnp.full((SEQC, TILED), -jnp.inf, F32)
                for zz in range(NZ):
                    one = lax.dot_general(kd[zz * NY + yy, :, cols], q, NT, preferred_element_type=F32)
                    s = jnp.where((lane // RD == zz) & seen, one, s)
                extra = lax.dot_general(ksd[:, cols], q, NT, preferred_element_type=F32)
                jobs.append((part, yy, c, s, jnp.where(own, extra, -jnp.inf)))
        ready = []
        for part, yy, c, s, extra in jobs:
            m = jnp.max(jnp.maximum(s, extra), axis=0, keepdims=True)
            w = jnp.exp2((s - m) * EXPC)
            we = jnp.exp2((extra - m) * EXPC)
            total = jnp.sum(w + we, axis=0, keepdims=True)
            for zz in range(NZ):
                b = zz * NY + yy
                dsend[b, 4 + c : 5 + c, :] = m
                dsend[b, 6 + c : 7 + c, :] = total
            ready.append((part, yy, c, w, we))
        for part, yy, c, w, we in ready:
            out = jnp.dot(vse[...], we.astype(BF16), preferred_element_type=F32)
            for zz in range(NZ):
                some = jnp.where(lane // RD == zz, w, 0.0).astype(BF16)
                out = out + jnp.dot(
                    vtd[part, :, zz * SEQC : (zz + 1) * SEQC], some, preferred_element_type=F32
                )
            out = out.T
            for zz in range(NZ):
                for hh in range(2):
                    dsend[zz * NY + yy, 2 * c + hh : 2 * c + hh + 1, :] = out[
                        RD * zz : RD * zz + 1, hh * 128 : (hh + 1) * 128
                    ]

    loads[7].wait()
    loads[8].wait()

    events = (
        ((z_relay, 0, 1), (z_relay, 0, 2), (z_relay, 0, 3), (z_send, 1)),
        ((y_relay, 0, 0), (y_relay, 0, 1), (y_relay, 0, 2), (y_relay, 0, 3), (z_relay, 1, 0), (z_relay, 1, 1)),
        ((z_relay, 1, 2), (z_relay, 1, 3), (z_send, 2)),
        ((h_wait, 0), (y_relay, 1, 0), (y_relay, 1, 1)),
        ((y_relay, 1, 2), (y_relay, 1, 3), (z_relay, 2, 0), (z_relay, 2, 1)),
        ((stats_send, 0), (z_relay, 2, 2), (z_relay, 2, 3), (z_send, 3)),
        (),
        ((h_wait, 1), (y_relay, 2, 0), (y_relay, 2, 1)),
        ((stats_own, 0), (y_relay, 2, 2), (y_relay, 2, 3), (z_wait_y_send, 3)),
        ((stats_send, 1),),
        ((y_wait_fwd, 3),),
        ((h_wait, 2),),
        ((rs_first, 0), (stats_own, 1)),
        ((stats_send, 2),),
        ((h_wait, 3), (rs_second, 0)),
        (),
    )

    @pl.loop(0, COUNT + 4)
    def _(t):
        for step, jobs in enumerate(events):
            if jobs:

                def run(jobs=jobs):
                    for work, *args in jobs:
                        work(*args)

                pl.when(t == step)(run)
        pl.when(t < COUNT + 2)(functools.partial(piece_step, t))
        pl.when(t >= COUNT + 2)(functools.partial(decode_step, t))

    def d_copy(target):
        return rcopy(dsend.at[target], drecv.at[me], ds.at[0], dr.at[0], target)

    @pl.loop(1, NKV)
    def _(d):
        d_copy((me + d) % NKV).start()

    drecv[me] = dsend[me]

    def d_all():
        most = drecv.at[pl.ds(0, NKV - 1)]
        return rcopy(most, most, ds.at[0], dr.at[0], z * NY + yp)

    def decode_row():
        d_all().wait_recv()
        mine = lax.broadcasted_iota(jnp.int32, (NKV, 128), 1) == RD * z
        parts = []
        for c in range(2):
            pick = lambda at: jnp.sum(jnp.where(mine, drecv[:, at, :], 0.0), axis=1, keepdims=True)
            m = pick(4 + c)
            scale = jnp.exp2((m - jnp.max(m, axis=0, keepdims=True)) * EXPC)
            norm = jnp.sum(pick(6 + c) * scale, axis=0, keepdims=True)
            parts.append(
                [jnp.sum(drecv[:, 2 * c + hh, :] * scale, axis=0, keepdims=True) / norm for hh in range(2)]
            )
        for hh in range(2):
            mixed[ROWS : ROWS + 1, hh * 128 : (hh + 1) * 128] = parts[0][hh] - mix[0] * parts[1][hh]

    stats_own(2)
    rs_first(1)
    rs_third(0)
    rs_second(1)
    rs_first(2)
    rs_last(0)
    project_out(0)
    rs_second(2)
    rs_third(1)
    tp_first(0)
    decode_row()
    project_out(3)
    rs_third(2)
    rs_last(1)
    project_out(1)
    tp_first(3)
    tp_first(1)
    rs_last(2)
    project_out(2)
    tp_last(0)
    tp_last(3)
    tp_first(2)
    tp_last(1)
    tp_last(2)

    for j in range(4):
        z_all(j).wait_send()
        p_copy(j).wait_send()
        u_all(j).wait_send()
        for side in (0, 1):
            y_copy(j, side).wait_send()
            half = half_of(qtile(j, y), j, side)
            rcopy(half, half, hs.at[j, side], hr.at[j, side], z * NY + yp).wait_send()
    for j in range(CHUNKS):
        w_all(j).wait_send()
        for side in (0, 1):
            x_copy(j, side).wait_send()
            f_copy(j, side).wait_send()
        for yt in range(NY):

            @pl.when(STAT_Z[j] * NY + yt != me)
            def _():
                s_copy(j, yt).wait_send()

        @pl.when(z == STAT_Z[j])
        def _():
            most = srecv.at[j, pl.ds(0, NKV - 1)]
            rcopy(most, most, rs.at[j], sr.at[j], z * NY + yp).wait_send()

    d_all().wait_send()


def attention(tok, step_tok, in_gain, wq, wk, wv, kp, vp, kd, vd, wo, gain, prompt_len, step_lens, mix):
    vmem = pl.BlockSpec(memory_space=pltpu.VMEM)
    anyw = pl.BlockSpec(memory_space=pl.ANY)
    smem = pl.BlockSpec(memory_space=pltpu.SMEM)
    dma = pltpu.SemaphoreType.DMA
    V = pltpu.VMEM
    nt = CHUNKS * NY
    return pl.pallas_call(
        attend,
        out_shape=jax.ShapeDtypeStruct((PADDED, OUTB + 2 * DV), BF16),
        in_specs=[anyw, vmem, vmem] + [anyw] * 8 + [vmem, smem, smem, smem],
        out_specs=vmem,
        scratch_shapes=[
            V((ROWS, D), BF16),
            V((PADDED, D), BF16),
            V((2 * D, DH), BF16),
            V((2 * D, DH), BF16),
            V((D, 2 * DH), BF16),
            V((D, DV), BF16),
            V((DV, D), BF16),
            V((2 * CACHE + 2 * NKV * SEQC, DH), BF16),
            V((512, DH), F32),
            V((KEYS, 2 * DH), BF16),
            V((CACHE, DV), BF16),
            V((DV, KEYS), BF16),
            V((NKV, SEQC, 2 * DH), BF16),
            V((NKV, SEQC, DV), BF16),
            V((2, DV, NZ * SEQC), BF16),
            V((SEQC, 2 * DH), BF16),
            V((DV, SEQC), BF16),
            V((nt, TILE, 2 * DH), BF16),
            V((NY, TILED, 2 * DH), BF16),
            V((CACHE // 2, 128), F32),
            V((2, KEYS, TILE), F32),
            V((2, KEYS, TILE), BF16),
            V((2, 8, TILE), F32),
            V((nt + 1, 2, DV, TILE), F32),
            V((nt + 1, 8, 128), F32),
            V((CHUNKS, NKV, 8, 128), F32),
            V((CHUNKS, 8, 128), F32),
            V((nt, 8, 128), F32),
            V((NKV, 8, 128), F32),
            V((NKV, 8, 128), F32),
            V((nt, TILE, DV), BF16),
            V((CHUNKS, 2, TILE // 2, DV), BF16),
            V((CHUNKS, 2, TILE, DV), BF16),
            V((CHUNKS, TILE, DV), F32),
            V((CHUNKS, TILE, DV), BF16),
            V((CHUNKS, NZ - 1, R, DV), BF16),
            V((PADDED, DV), F32),
            V((2, NX, PADDED, OUTB), BF16),
            V((NX, PADDED, OUTB), BF16),
            V((NX, PADDED, OUTB), BF16),
            V((NX - 1, PADDED, OUTB), BF16),
            dma((9,)),
            dma((4,)), dma((4, 4)),
            dma((4, 2)), dma((4, 4)),
            dma((4, 2)), dma((4, 2)),
            dma((3, NY)), dma((3,)),
            dma((3,)), dma((3, NY)),
            dma((3, 2)), dma((3, 2)),
            dma((3, 2)), dma((3, 2)),
            dma((3,)), dma((3,)),
            dma((1,)), dma((1,)),
            dma((4,)), dma((4,)),
            dma((4,)), dma((4,)),
        ],
        compiler_params=pltpu.CompilerParams(
            collective_id=0, has_side_effects=True, vmem_limit_bytes=62 << 20
        ),
        name="attend",
    )(tok, step_tok, in_gain, wq, wk, wv, kp, vp, kd, vd, wo, gain, prompt_len, step_lens, mix)


def split_outputs(all_ref, piece_ref, step_ref, pk_ref, pv_ref, sk_ref, sv_ref, flat):
    piece_ref[...] = all_ref[:ROWS, :OUTB]
    step_ref[...] = all_ref[ROWS : ROWS + 1, :OUTB]
    pv_ref[...] = all_ref[:ROWS, OUTB : OUTB + DV]
    sv_ref[...] = all_ref[ROWS : ROWS + 1, OUTB : OUTB + DV]
    for c in range(2):
        at = OUTB + DV + c * DH
        flat[pl.ds(c, PADDED, 2), :] = all_ref[:, at : at + DH].astype(F32)
    pk_ref[...] = flat[: 2 * ROWS, :].astype(BF16)
    sk_ref[...] = flat[2 * ROWS : 2 * ROWS + 2, :].astype(BF16)


def on_device(
    piece_tokens, step_tokens, in_gain, w_query, w_key, w_value, w_out, mix_ratio, out_gain,
    prompt_keys, prompt_values, step_cache_keys, step_cache_values, prompt_len, step_lens,
):
    together = attention(
        piece_tokens, step_tokens, in_gain.reshape(1, D),
        w_query.reshape(2 * D, DH), w_key.reshape(2 * D, DH), w_value.reshape(D, DV),
        prompt_keys.reshape(2 * CACHE, DH), prompt_values.reshape(CACHE, DV),
        step_cache_keys.reshape(2 * NKV * SEQC, DH), step_cache_values.reshape(NKV, SEQC, DV),
        w_out.reshape(DV, D), out_gain.reshape(1, DV), prompt_len, step_lens, mix_ratio,
    )
    shapes = ((ROWS, OUTB), (1, OUTB), (2 * ROWS, DH), (ROWS, DV), (2, DH), (1, DV))
    piece_out, step_out, piece_k, piece_v, step_k, step_v = pl.pallas_call(
        split_outputs,
        out_shape=tuple(jax.ShapeDtypeStruct(shape, BF16) for shape in shapes),
        scratch_shapes=[pltpu.VMEM((2 * PADDED, DH), F32)],
        name="split",
    )(together)
    return (
        piece_out, step_out,
        piece_k.reshape(ROWS, 1, 2, DH), piece_v.reshape(ROWS, 1, DV),
        step_k.reshape(1, 1, 2, DH), step_v.reshape(1, 1, DV),
    )


def solution(mesh):
    in_specs = (
        P("kv", None),
        P("kv", None),
        P(),
        P(None, "tp", None, None),
        P(None, "tp", None, None),
        P(None, "tp", None),
        P("tp", None, None),
        P("tp"),
        P(),
        P("kv", "tp", None, None),
        P("kv", "tp", None),
        P(None, "kv", "tp", None, None),
        P(None, "kv", "tp", None),
        P(),
        P(),
    )
    out_specs = (
        P("kv", "tp"),
        P("kv", "tp"),
        P("kv", "tp", None, None),
        P("kv", "tp", None),
        P("kv", "tp", None, None),
        P("kv", "tp", None),
    )
    return jax.shard_map(
        on_device, mesh=mesh, in_specs=in_specs, out_specs=out_specs, check_vma=False
    )
```

```python
import functools
import math

import jax
import jax.numpy as jnp
from jax import lax
from jax.experimental import pallas as pl
from jax.experimental.pallas import tpu as pltpu
from jax.sharding import PartitionSpec as P

EPS = 1e-06
OUT_SCALE = 0.8
NZ, NY, NKV, NX = 8, 4, 32, 4
D, OUTB = 4096, 512
ROWS = 96
CHUNKS = 3
R = ROWS // CHUNKS
RD = 16
TILE = NZ * R
COUNT = CHUNKS * NY
TILED = NZ * RD
CACHE = 2048
KEYS = CACHE + 128
SEQC = 128
DH, DV = 128, 256
PADDED = ROWS + RD
EXPC = DH ** (-0.5) * math.log2(math.e)
STAT_Z = (1, 4, 7)
BATCHES = ((0,), (1, 7), (2, 6), (3, 5, 4))
F32, BF16 = jnp.float32, jnp.bfloat16
NT = (((1,), (1,)), ((), ()))


def attend(
    tok_hbm, step_tok, in_gain, wq_hbm, wk_hbm, wv_hbm, kp_hbm, vp_hbm, kd_hbm, vd_hbm, wo_hbm,
    gain_ref, plen, slens, mix,
    out_ref,
    tok, normed, wq, wk, wdeint, wv, wo, kraw, kfloat, kbuf, vnat, vt, kd, vdn, vtd, ksd, vse, qall, qd,
    bias, sbuf, mrow, oacc,
    stat, srecv, ressend, res, dsend, drecv, comb, rh, rf, acc, accb, rz, mixed,
    term, tsum, pr, tf,
    load_sem, zs, zr, ys, yr, hs, hr, ss, sr, rs, rr, xs, xr, fs, fr, ws, wr, ds, dr,
    ps, ps_r, us, ur,
):
    me = lax.axis_index("kv")
    tp = lax.axis_index("tp")
    z = me // NY
    y = me % NY
    yp, ym, y2 = (y + 1) % NY, (y + 3) % NY, (y + 2) % NY
    x = tp // 2
    core = tp % 2
    xp, xm, x2 = (x + 1) % NX, (x + 3) % NX, (x + 2) % NX

    def at_kv(index):
        return {"kv": index}

    def rcopy(src, dst, s_sem, r_sem, target):
        return pltpu.make_async_remote_copy(
            src_ref=src, dst_ref=dst, send_sem=s_sem, recv_sem=r_sem,
            device_id=at_kv(target), device_id_type=pl.DeviceIdType.MESH,
        )

    def tcopy(src, dst, s_sem, r_sem, tx, tc):
        return pltpu.make_async_remote_copy(
            src_ref=src, dst_ref=dst, send_sem=s_sem, recv_sem=r_sem,
            device_id={"tp": tx * 2 + tc}, device_id_type=pl.DeviceIdType.MESH,
        )

    def rows_of(j):
        return R if j < CHUNKS else RD

    def qtile(j, yy):
        return qall.at[j * NY + yy] if j < CHUNKS else qd.at[yy]

    def ctile(j, yy):
        return comb.at[j * NY + yy]

    def zblock(view, zz, n):
        return view.at[pl.ds(pl.multiple_of(zz * n, n), n), :]

    loads = [
        pltpu.make_async_copy(tok_hbm, tok, load_sem.at[0]),
        pltpu.make_async_copy(wq_hbm, wq, load_sem.at[1]),
        pltpu.make_async_copy(wk_hbm, wk, load_sem.at[2]),
        pltpu.make_async_copy(wv_hbm, wv, load_sem.at[3]),
        pltpu.make_async_copy(kp_hbm, kraw.at[pl.ds(0, 2 * CACHE), :], load_sem.at[4]),
        pltpu.make_async_copy(vp_hbm, vnat, load_sem.at[5]),
        pltpu.make_async_copy(kd_hbm, kraw.at[pl.ds(2 * CACHE, 2 * NKV * SEQC), :], load_sem.at[6]),
        pltpu.make_async_copy(vd_hbm, vdn, load_sem.at[7]),
        pltpu.make_async_copy(wo_hbm, wo, load_sem.at[8]),
    ]
    for load in loads[:2]:
        load.start()

    barrier = pltpu.get_barrier_semaphore()

    @pl.loop(1, NKV)
    def _(d):
        pl.semaphore_signal(
            barrier, inc=1, device_id=at_kv((me + d) % NKV),
            device_id_type=pl.DeviceIdType.MESH,
        )

    for tx, tc in ((x, 1 - core), (xp, core), (x2, core), (xm, core)):
        pl.semaphore_signal(
            barrier, inc=1, device_id={"tp": tx * 2 + tc}, device_id_type=pl.DeviceIdType.MESH
        )

    def norm(rows):
        floats = rows.astype(F32)
        inv_rms = lax.rsqrt(jnp.mean(floats * floats, axis=-1, keepdims=True) + EPS)
        return (floats * inv_rms * in_gain[...]).astype(BF16)

    last = norm(step_tok[...])
    normed[ROWS:, :] = jnp.concatenate([last, jnp.zeros((RD - 1, D), BF16)], axis=0)
    loads[0].wait()
    for load in loads[2:]:
        load.start()

    @pl.loop(0, ROWS // 16)
    def _(b):
        rows = pl.ds(pl.multiple_of(b * 16, 16), 16)
        normed[rows, :] = norm(tok[rows, :])

    def split_maps(src, src_block, put):
        kfloat[...] = src[pl.ds(pl.multiple_of(src_block * 512, 512), 512), :].astype(F32)
        for c in range(2):
            put(c, kfloat[pl.ds(c, 256, 2), :].astype(BF16))

    def projected(weights):
        @pl.loop(0, D // 256)
        def _(b):
            def put(c, flat):
                rows = pl.ds(pl.multiple_of(b * 256, 256), 256)
                wdeint[rows, c * DH : (c + 1) * DH] = flat

            split_maps(weights, b, put)

        return jnp.dot(normed[...], wdeint[...], preferred_element_type=F32).astype(BF16)

    loads[1].wait()
    queries = projected(wq)
    for j in range(4):
        n = rows_of(j)
        lo = j * R if j < CHUNKS else ROWS
        mine = qtile(j, y)
        mine[pl.ds(pl.multiple_of(z * n, n), n), :] = queries[lo : lo + n, :]

    def batch_sem(d):
        return {0: 0, 1: 1, 7: 1, 2: 2, 6: 2}.get(d, 3)

    def origin(d):
        return (z + NZ - d) % NZ

    def z_copy(j, d):
        block = zblock(qtile(j, y), z, rows_of(j))
        sem = zr.at[j, batch_sem(d)] if j < CHUNKS else zr.at[j, 0]
        return rcopy(block, block, zs.at[j], sem, ((z + d) % NZ) * NY + y)

    def z_some(j, count, sem):
        some = qtile(j, y).at[pl.ds(0, count * rows_of(j)), :]
        return rcopy(some, some, zs.at[j], sem, z * NY + yp)

    def z_all(j):
        return z_some(j, NZ - 1, zr.at[j, 0])

    def z_send(j):
        for d in (4, 3, 5, 2, 6, 1, 7):
            z_copy(j, d).start()

    def side_kv(side):
        return z * NY + (yp if side == 0 else ym)

    def z_relay(j, k):
        if k > 0:
            z_some(j, len(BATCHES[k]), zr.at[j, k]).wait_recv()
        for d in BATCHES[k]:
            block = zblock(qtile(j, y), origin(d), R)
            for side in (0, 1):
                rcopy(block, block, ys.at[j], yr.at[j, k], side_kv(side)).start()

    def y_relay(j, k):
        z_some(j, 2 * len(BATCHES[k]), yr.at[j, k]).wait_recv()
        for side in (0, 1):
            for d in BATCHES[k]:
                if (side == 0) == (d < NZ // 2):
                    block = zblock(qtile(j, ym if side == 0 else yp), origin(d), R)
                    rcopy(block, block, hs.at[j], hr.at[j], side_kv(side)).start()

    pl.semaphore_wait(barrier, NKV - 1 + 4)
    z_send(0)
    z_relay(0, 0)

    loads[2].wait()
    keys = projected(wk)
    out_ref[:, OUTB + DV :] = keys
    loads[3].wait()
    values = jnp.dot(normed[...], wv[...], preferred_element_type=F32).astype(BF16)
    out_ref[:, OUTB : OUTB + DV] = values

    kbuf[CACHE : CACHE + ROWS, :] = keys[:ROWS, :]
    kbuf[CACHE + ROWS :, :] = jnp.zeros((KEYS - CACHE - ROWS, 2 * DH), BF16)
    ksd[:RD, :] = keys[ROWS:, :]
    ksd[RD:, :] = jnp.zeros((SEQC - RD, 2 * DH), BF16)
    tail = jnp.concatenate([values[:ROWS, :], jnp.zeros((128 - ROWS, DV), BF16)], axis=0)
    vt[:, CACHE:] = tail.T
    tail = jnp.concatenate([values[ROWS:, :], jnp.zeros((128 - RD, DV), BF16)], axis=0)
    vse[...] = tail.T
    half = CACHE // 2
    place = me * CACHE + half + lax.broadcasted_iota(jnp.int32, (half, 128), 0)
    bias[...] = jnp.where(place < plen[0], 0.0, -jnp.inf).astype(F32)
    mixed[...] = jnp.zeros((PADDED, DV), F32)
    loads[4].wait()
    loads[5].wait()

    @pl.loop(0, CACHE // 256)
    def _(b):
        def put(c, flat):
            kbuf[pl.ds(pl.multiple_of(b * 256, 256), 256), c * DH : (c + 1) * DH] = flat

        split_maps(kraw, b, put)

    for b in range(CACHE // 256):
        vt[:, b * 256 : (b + 1) * 256] = vnat[b * 256 : (b + 1) * 256, :].T
    loads[6].wait()

    @pl.loop(0, NKV // 2)
    def _(b):
        def put(c, flat):
            for part in range(2):
                kd[2 * b + part, :, c * DH : (c + 1) * DH] = flat[part * SEQC : (part + 1) * SEQC]

        split_maps(kraw, 2 * CACHE // 512 + b, put)

    def z_wait_y_send(j):
        z_all(j).wait_recv()
        y_copy(j, 0).start()
        y_copy(j, 1).start()

    def y_copy(j, side):
        tile = qtile(j, y)
        sem = yr.at[j, side]
        return rcopy(tile, tile, ys.at[j], sem, side_kv(side))

    def half_of(view, j, side):
        h = NZ * rows_of(j) // 2
        return view.at[pl.ds(side * h, h), :]

    def h_copy(j, side):
        part = half_of(qtile(j, ym if side == 0 else yp), j, side)
        return rcopy(part, part, hs.at[j], hr.at[j], side_kv(side))

    def y_wait_fwd(j):
        for side in (0, 1):
            tile = qtile(j, ym if side == 0 else yp)
            rcopy(tile, tile, ys.at[j], yr.at[j, side], z * NY + yp).wait_recv()
            h_copy(j, side).start()

    def h_all(j):
        tile = qtile(j, y2)
        return rcopy(tile, tile, hs.at[j], hr.at[j], z * NY + yp)

    def h_wait(j):
        h_all(j).wait_recv()

    def y_all(j):
        two = qall.at[pl.ds(0, 2)] if j < CHUNKS else qd.at[pl.ds(0, 2)]
        return rcopy(two, two, ys.at[j], yr.at[j, 0], z * NY + yp)

    def s_copy(j, yt):
        return rcopy(
            stat.at[j * NY + yt], srecv.at[j, me], ss.at[j], sr.at[j], STAT_Z[j] * NY + yt
        )

    def s_some(j, count):
        some = stat.at[pl.ds(0, count)]
        return rcopy(some, some, ss.at[j], rr.at[j], z * NY + yp)

    def stats_send(j):
        for yt in range(NY):
            target = STAT_Z[j] * NY + yt

            @pl.when(target != me)
            def _():
                s_copy(j, yt).start()

            @pl.when(target == me)
            def _():
                srecv[j, me] = stat[j * NY + yt]

    def r_copy(j, target):
        return rcopy(ressend.at[j], res.at[j * NY + y], rs.at[j], rr.at[j], target)

    def stats_own(j):
        @pl.when(z == STAT_Z[j])
        def _():
            most = srecv.at[j, pl.ds(0, NKV - 1)]
            rcopy(most, most, rs.at[j], sr.at[j], z * NY + yp).wait_recv()
            every = srecv[j]
            best = jnp.max(every[:, 0:4, :], axis=0)
            norm = jnp.sum(every[:, 4:8, :] * jnp.exp2((every[:, 0:4, :] - best[None]) * EXPC), axis=0)
            both = jnp.concatenate([best, 1.0 / norm], axis=0)
            ressend[j] = both
            res[j * NY + y] = both

            @pl.loop(1, NKV)
            def _(d):
                r_copy(j, (me + d) % NKV).start()

    def stats_wait(j):
        @pl.when(z == STAT_Z[j])
        def _():
            s_some(j, NY - 1).wait_recv()

        @pl.when(z != STAT_Z[j])
        def _():
            s_some(j, NY).wait_recv()

    def combine(j, yy):
        tt = j * NY + yy
        factors = []
        for c in range(2):
            pick = lambda ref, lo: jnp.concatenate(
                [ref[tt, lo + 2 * c + hh : lo + 2 * c + hh + 1, :] for hh in range(2)], axis=1
            )
            factors.append(jnp.exp2((pick(stat, 0) - pick(res, 0)) * EXPC) * pick(res, 4))
        both = oacc[tt, 0] * factors[0] - oacc[tt, 1] * (factors[1] * mix[0])
        comb[tt] = both.T.astype(BF16)

    def x_copy(j, side):
        part = half_of(ctile(j, y2), j, side)
        return rcopy(part, rh.at[j, side], xs.at[j], xr.at[j, side], z * NY + (yp if side == 0 else ym))

    def f_copy(j, side):
        tile = ctile(j, yp if side == 0 else ym)
        return rcopy(tile, rf.at[j, side], fs.at[j], fr.at[j, side], z * NY + (yp if side == 0 else ym))

    def rs_first(j):
        stats_wait(j)
        combine(j, y2)
        for side in (0, 1):
            x_copy(j, side).start()

        @pl.loop(1, NY)
        def _(i):
            combine(j, (y2 + i) % NY)

    def rs_second(j):
        for side in (0, 1):
            x_copy(j, side).wait_recv()
            part = half_of(ctile(j, yp if side == 0 else ym), j, side)
            part[...] = (part[...].astype(F32) + rh[j, side].astype(F32)).astype(BF16)
            f_copy(j, side).start()

    def w_copy(j, d):
        zt = (z + d) % NZ
        return rcopy(zblock(accb.at[j], zt, R), rz.at[j, d - 1], ws.at[j], wr.at[j], zt * NY + y)

    def w_all(j):
        return rcopy(rz.at[j], rz.at[j], ws.at[j], wr.at[j], z * NY + yp)

    def rs_third(j):
        for side in (0, 1):
            f_copy(j, side).wait_recv()
        total = comb[j * NY + y].astype(F32) + rf[j, 0].astype(F32) + rf[j, 1].astype(F32)
        accb[j] = total.astype(BF16)
        acc[j] = total
        for d in (4, 3, 5, 2, 6, 1, 7):
            w_copy(j, d).start()

    def rs_last(j):
        total = acc[j, pl.ds(pl.multiple_of(z * R, R), R), :]
        w_all(j).wait_recv()
        for d in range(NZ - 1):
            total = total + rz[j, d].astype(F32)
        mixed[j * R : (j + 1) * R, :] = total

    def span(j):
        return slice(j * R, j * R + rows_of(j))

    def p_copy(j):
        return tcopy(
            term.at[1 - core, :, span(j), :], pr.at[:, span(j), :], ps.at[j], ps_r.at[j], x, 1 - core
        )

    def project_out(j):
        n = rows_of(j)
        total = mixed[span(j), :]
        inv_rms = lax.rsqrt(jnp.mean(total * total, axis=-1, keepdims=True) + EPS)
        head = (total * inv_rms * gain_ref[...] * OUT_SCALE).astype(BF16)
        for tc in (1 - core, core):
            for tx in range(NX):
                at = pl.multiple_of((tx * 2 + tc) * OUTB, OUTB)
                one = jnp.dot(head, wo[:, pl.ds(at, OUTB)], preferred_element_type=F32)
                term[tc, tx, span(j), :] = one.astype(BF16)
            if tc is not core:
                p_copy(j).start()

    def u_copy(j, d):
        to = (x + d) % NX
        return tcopy(tsum.at[to, span(j), :], tf.at[d - 1, span(j), :], us.at[j], ur.at[j], to, core)

    def u_all(j):
        some = tf.at[:, span(j), :]
        return tcopy(some, some, us.at[j], ur.at[j], xp, core)

    def tp_first(j):
        p_copy(j).wait_recv()
        for tx in range(NX):
            both = term[core, tx, span(j), :].astype(F32) + pr[tx, span(j), :].astype(F32)
            tsum[tx, span(j), :] = both.astype(BF16)
        for d in (2, 1, 3):
            u_copy(j, d).start()

    def tp_last(j):
        u_all(j).wait_recv()
        total = term[core, x, span(j), :].astype(F32) + pr[x, span(j), :].astype(F32)
        for d in range(NX - 1):
            total = total + tf[d, span(j), :].astype(F32)
        out_ref[span(j), :OUTB] = total.astype(BF16)

    KB = [(b * 256, 256) for b in range(CACHE // 256)] + [(CACHE, 128)]

    def tile_of(t):
        i = t % NY
        yy = (y + jnp.where(i == 2, 3, jnp.where(i == 3, 2, i))) % NY
        return t // NY, yy, (t // NY) * NY + yy

    def piece_step(t, scores=True):
        j, yy, ta = tile_of(jnp.minimum(t, COUNT - 1))
        tb = jnp.where(t >= 1, tile_of(jnp.maximum(t - 1, 0))[2], COUNT)
        lane = lax.broadcasted_iota(jnp.int32, (128, TILE), 1)
        row = lax.broadcasted_iota(jnp.int32, (128, TILE), 0)
        row_place = ((lane // R) * NY + yy) * ROWS + R * j + lane % R
        fresh_ok = (row < ROWS) & (me * ROWS + row <= row_place)
        for c in range(2):
            cols = slice(c * DH, (c + 1) * DH)
            q = qall[ta, :, cols]
            m = mrow[c, 0:1, :]
            top = jnp.full((8, TILE), -jnp.inf, F32)
            total = jnp.zeros((8, TILE), F32)
            out = jnp.zeros((DV, TILE), F32)
            for at, size in KB:
                w = jnp.exp2((sbuf[c, at : at + size, :] - m) * EXPC)
                total = total + jnp.sum(w.reshape(size // 8, 8, TILE), axis=0)
                out = out + jnp.dot(
                    vt[:, at : at + size], w.astype(BF16), preferred_element_type=F32
                )
                if not scores:
                    continue
                s = lax.dot_general(kbuf[at : at + size, cols], q, NT, preferred_element_type=F32)
                if at == CACHE:
                    s = jnp.where(fresh_ok, s, -jnp.inf)
                elif at >= half:
                    b = bias[at - half : at - half + size, :]
                    s = s + jnp.concatenate([b, b], axis=1)
                sbuf[c, at : at + size, :] = s
                top = jnp.maximum(top, jnp.max(s.reshape(size // 8, 8, TILE), axis=0))
            oacc[tb, c] = out
            total = jnp.sum(total, axis=0, keepdims=True)
            for hh in range(2):
                stat[tb, 2 * c + hh : 2 * c + hh + 1, :] = m[:, hh * 128 : (hh + 1) * 128]
                stat[tb, 4 + 2 * c + hh : 5 + 2 * c + hh, :] = total[:, hh * 128 : (hh + 1) * 128]
            if scores:
                mrow[c, 0:1, :] = jnp.max(top, axis=0, keepdims=True)

    def decode_step(t):
        lane = lax.broadcasted_iota(jnp.int32, (SEQC, TILED), 1)
        row = lax.broadcasted_iota(jnp.int32, (SEQC, TILED), 0)
        jobs = []
        for part in range(2):
            yy = 2 * (t - COUNT - 1) + part
            q2 = qd[yy]
            own = (lane // RD == jnp.where(yy == y, z, NZ)) & (row == 0)
            limit = jnp.zeros((SEQC, TILED), jnp.int32)
            for zz in range(NZ):
                vtd[part, :, zz * SEQC : (zz + 1) * SEQC] = vdn[zz * NY + yy].T
                limit = jnp.where(lane // RD == zz, slens[zz * NY + yy], limit)
            seen = me * SEQC + row < limit
            for c in range(2):
                cols = slice(c * DH, (c + 1) * DH)
                q = q2[:, cols]
                s = jnp.full((SEQC, TILED), -jnp.inf, F32)
                for zz in range(NZ):
                    one = lax.dot_general(kd[zz * NY + yy, :, cols], q, NT, preferred_element_type=F32)
                    s = jnp.where((lane // RD == zz) & seen, one, s)
                extra = lax.dot_general(ksd[:, cols], q, NT, preferred_element_type=F32)
                jobs.append((part, yy, c, s, jnp.where(own, extra, -jnp.inf)))
        ready = []
        for part, yy, c, s, extra in jobs:
            m = jnp.max(jnp.maximum(s, extra), axis=0, keepdims=True)
            w = jnp.exp2((s - m) * EXPC)
            we = jnp.exp2((extra - m) * EXPC)
            total = jnp.sum(w + we, axis=0, keepdims=True)
            for zz in range(NZ):
                b = zz * NY + yy
                dsend[b, 4 + c : 5 + c, :] = m
                dsend[b, 6 + c : 7 + c, :] = total
            ready.append((part, yy, c, w, we))
        for part, yy, c, w, we in ready:
            out = jnp.dot(vse[...], we.astype(BF16), preferred_element_type=F32)
            for zz in range(NZ):
                some = jnp.where(lane // RD == zz, w, 0.0).astype(BF16)
                out = out + jnp.dot(
                    vtd[part, :, zz * SEQC : (zz + 1) * SEQC], some, preferred_element_type=F32
                )
            out = out.T
            for zz in range(NZ):
                for hh in range(2):
                    dsend[zz * NY + yy, 2 * c + hh : 2 * c + hh + 1, :] = out[
                        RD * zz : RD * zz + 1, hh * 128 : (hh + 1) * 128
                    ]

    loads[7].wait()
    loads[8].wait()

    events = (
        ((z_relay, 0, 1), (z_relay, 0, 2), (z_relay, 0, 3), (z_send, 1)),
        ((y_relay, 0, 0), (y_relay, 0, 1), (y_relay, 0, 2), (y_relay, 0, 3), (z_relay, 1, 0), (z_relay, 1, 1)),
        ((z_relay, 1, 2), (z_relay, 1, 3), (z_send, 2)),
        ((h_wait, 0), (y_relay, 1, 0), (y_relay, 1, 1)),
        ((z_relay, 2, 0), (z_relay, 2, 1)),
        ((stats_send, 0), (y_relay, 1, 2), (y_relay, 1, 3), (z_relay, 2, 2), (z_relay, 2, 3), (z_send, 3)),
        (),
        ((h_wait, 1), (y_relay, 2, 0), (y_relay, 2, 1)),
        ((stats_own, 0), (y_relay, 2, 2), (y_relay, 2, 3), (z_wait_y_send, 3)),
        ((stats_send, 1),),
        (),
        ((h_wait, 2), (y_wait_fwd, 3)),
        ((rs_first, 0), (stats_own, 1)),
        ((stats_send, 2), (h_wait, 3)),
        ((rs_second, 0),),
    )

    @pl.loop(0, COUNT + 3)
    def _(t):
        for step, jobs in enumerate(events):
            if jobs:

                def run(jobs=jobs):
                    for work, *args in jobs:
                        work(*args)

                pl.when(t == step)(run)
        pl.when(t < COUNT)(functools.partial(piece_step, t))
        pl.when(t == COUNT)(functools.partial(piece_step, t, False))
        pl.when(t >= COUNT + 1)(functools.partial(decode_step, t))

    def d_copy(target):
        return rcopy(dsend.at[target], drecv.at[me], ds.at[0], dr.at[0], target)

    @pl.loop(1, NKV)
    def _(d):
        d_copy((me + d) % NKV).start()

    drecv[me] = dsend[me]

    def d_all():
        most = drecv.at[pl.ds(0, NKV - 1)]
        return rcopy(most, most, ds.at[0], dr.at[0], z * NY + yp)

    def decode_row():
        d_all().wait_recv()
        mine = lax.broadcasted_iota(jnp.int32, (NKV, 128), 1) == RD * z
        parts = []
        for c in range(2):
            pick = lambda at: jnp.sum(jnp.where(mine, drecv[:, at, :], 0.0), axis=1, keepdims=True)
            m = pick(4 + c)
            scale = jnp.exp2((m - jnp.max(m, axis=0, keepdims=True)) * EXPC)
            norm = jnp.sum(pick(6 + c) * scale, axis=0, keepdims=True)
            parts.append(
                [jnp.sum(drecv[:, 2 * c + hh, :] * scale, axis=0, keepdims=True) / norm for hh in range(2)]
            )
        for hh in range(2):
            mixed[ROWS : ROWS + 1, hh * 128 : (hh + 1) * 128] = parts[0][hh] - mix[0] * parts[1][hh]

    rs_first(1)
    stats_own(2)
    rs_third(0)
    rs_first(2)
    rs_second(1)
    rs_last(0)
    project_out(0)
    rs_second(2)
    rs_third(1)
    decode_row()
    project_out(3)
    tp_first(0)
    rs_third(2)
    rs_last(1)
    project_out(1)
    tp_first(3)
    tp_first(1)
    rs_last(2)
    project_out(2)
    tp_last(0)
    tp_last(3)
    tp_first(2)
    tp_last(1)
    tp_last(2)

    for j in range(4):
        z_all(j).wait_send()
        y_all(j).wait_send()
        h_all(j).wait_send()
        p_copy(j).wait_send()
        u_all(j).wait_send()
    for j in range(CHUNKS):
        w_all(j).wait_send()
        rcopy(rf.at[j], rf.at[j], fs.at[j], fr.at[j, 0], z * NY + yp).wait_send()
        rcopy(rh.at[j], rh.at[j], xs.at[j], xr.at[j, 0], z * NY + yp).wait_send()

        @pl.when(z == STAT_Z[j])
        def _():
            most = srecv.at[j, pl.ds(0, NKV - 1)]
            rcopy(most, most, rs.at[j], sr.at[j], z * NY + yp).wait_send()
            s_some(j, NY - 1).wait_send()

        @pl.when(z != STAT_Z[j])
        def _():
            s_some(j, NY).wait_send()

    d_all().wait_send()


def attention(tok, step_tok, in_gain, wq, wk, wv, kp, vp, kd, vd, wo, gain, prompt_len, step_lens, mix):
    vmem = pl.BlockSpec(memory_space=pltpu.VMEM)
    anyw = pl.BlockSpec(memory_space=pl.ANY)
    smem = pl.BlockSpec(memory_space=pltpu.SMEM)
    dma = pltpu.SemaphoreType.DMA
    V = pltpu.VMEM
    nt = CHUNKS * NY
    return pl.pallas_call(
        attend,
        out_shape=jax.ShapeDtypeStruct((PADDED, OUTB + 2 * DV), BF16),
        in_specs=[anyw, vmem, vmem] + [anyw] * 8 + [vmem, smem, smem, smem],
        out_specs=vmem,
        scratch_shapes=[
            V((ROWS, D), BF16),
            V((PADDED, D), BF16),
            V((2 * D, DH), BF16),
            V((2 * D, DH), BF16),
            V((D, 2 * DH), BF16),
            V((D, DV), BF16),
            V((DV, D), BF16),
            V((2 * CACHE + 2 * NKV * SEQC, DH), BF16),
            V((512, DH), F32),
            V((KEYS, 2 * DH), BF16),
            V((CACHE, DV), BF16),
            V((DV, KEYS), BF16),
            V((NKV, SEQC, 2 * DH), BF16),
            V((NKV, SEQC, DV), BF16),
            V((2, DV, NZ * SEQC), BF16),
            V((SEQC, 2 * DH), BF16),
            V((DV, SEQC), BF16),
            V((nt, TILE, 2 * DH), BF16),
            V((NY, TILED, 2 * DH), BF16),
            V((CACHE // 2, 128), F32),
            V((2, KEYS, TILE), F32),
            V((2, 8, TILE), F32),
            V((nt + 1, 2, DV, TILE), F32),
            V((nt + 1, 8, 128), F32),
            V((CHUNKS, NKV, 8, 128), F32),
            V((CHUNKS, 8, 128), F32),
            V((nt, 8, 128), F32),
            V((NKV, 8, 128), F32),
            V((NKV, 8, 128), F32),
            V((nt, TILE, DV), BF16),
            V((CHUNKS, 2, TILE // 2, DV), BF16),
            V((CHUNKS, 2, TILE, DV), BF16),
            V((CHUNKS, TILE, DV), F32),
            V((CHUNKS, TILE, DV), BF16),
            V((CHUNKS, NZ - 1, R, DV), BF16),
            V((PADDED, DV), F32),
            V((2, NX, PADDED, OUTB), BF16),
            V((NX, PADDED, OUTB), BF16),
            V((NX, PADDED, OUTB), BF16),
            V((NX - 1, PADDED, OUTB), BF16),
            dma((9,)),
            dma((4,)), dma((4, 4)),
            dma((4,)), dma((4, 4)),
            dma((4,)), dma((4,)),
            dma((3,)), dma((3,)),
            dma((3,)), dma((3,)),
            dma((3,)), dma((3, 2)),
            dma((3,)), dma((3, 2)),
            dma((3,)), dma((3,)),
            dma((1,)), dma((1,)),
            dma((4,)), dma((4,)),
            dma((4,)), dma((4,)),
        ],
        compiler_params=pltpu.CompilerParams(
            collective_id=0, has_side_effects=True, vmem_limit_bytes=62 << 20
        ),
        name="attend",
    )(tok, step_tok, in_gain, wq, wk, wv, kp, vp, kd, vd, wo, gain, prompt_len, step_lens, mix)


def split_outputs(all_ref, piece_ref, step_ref, pk_ref, pv_ref, sk_ref, sv_ref, flat):
    piece_ref[...] = all_ref[:ROWS, :OUTB]
    step_ref[...] = all_ref[ROWS : ROWS + 1, :OUTB]
    pv_ref[...] = all_ref[:ROWS, OUTB : OUTB + DV]
    sv_ref[...] = all_ref[ROWS : ROWS + 1, OUTB : OUTB + DV]
    for c in range(2):
        at = OUTB + DV + c * DH
        flat[pl.ds(c, PADDED, 2), :] = all_ref[:, at : at + DH].astype(F32)
    pk_ref[...] = flat[: 2 * ROWS, :].astype(BF16)
    sk_ref[...] = flat[2 * ROWS : 2 * ROWS + 2, :].astype(BF16)


def on_device(
    piece_tokens, step_tokens, in_gain, w_query, w_key, w_value, w_out, mix_ratio, out_gain,
    prompt_keys, prompt_values, step_cache_keys, step_cache_values, prompt_len, step_lens,
):
    together = attention(
        piece_tokens, step_tokens, in_gain.reshape(1, D),
        w_query.reshape(2 * D, DH), w_key.reshape(2 * D, DH), w_value.reshape(D, DV),
        prompt_keys.reshape(2 * CACHE, DH), prompt_values.reshape(CACHE, DV),
        step_cache_keys.reshape(2 * NKV * SEQC, DH), step_cache_values.reshape(NKV, SEQC, DV),
        w_out.reshape(DV, D), out_gain.reshape(1, DV), prompt_len, step_lens, mix_ratio,
    )
    shapes = ((ROWS, OUTB), (1, OUTB), (2 * ROWS, DH), (ROWS, DV), (2, DH), (1, DV))
    piece_out, step_out, piece_k, piece_v, step_k, step_v = pl.pallas_call(
        split_outputs,
        out_shape=tuple(jax.ShapeDtypeStruct(shape, BF16) for shape in shapes),
        scratch_shapes=[pltpu.VMEM((2 * PADDED, DH), F32)],
        name="split",
    )(together)
    return (
        piece_out, step_out,
        piece_k.reshape(ROWS, 1, 2, DH), piece_v.reshape(ROWS, 1, DV),
        step_k.reshape(1, 1, 2, DH), step_v.reshape(1, 1, DV),
    )


def solution(mesh):
    in_specs = (
        P("kv", None),
        P("kv", None),
        P(),
        P(None, "tp", None, None),
        P(None, "tp", None, None),
        P(None, "tp", None),
        P("tp", None, None),
        P("tp"),
        P(),
        P("kv", "tp", None, None),
        P("kv", "tp", None),
        P(None, "kv", "tp", None, None),
        P(None, "kv", "tp", None),
        P(),
        P(),
    )
    out_specs = (
        P("kv", "tp"),
        P("kv", "tp"),
        P("kv", "tp", None, None),
        P("kv", "tp", None),
        P("kv", "tp", None, None),
        P("kv", "tp", None),
    )
    return jax.shard_map(
        on_device, mesh=mesh, in_specs=in_specs, out_specs=out_specs, check_vma=False
    )
```
